512 devices in a mesh: sp: 128 (over z, y, core), tp: 4 (over x).
Axes of the slice: x: 4, y: 8, z: 8, core: 2. Of those that a mesh axis runs over, the one named last changes fastest.
Arguments:
- tokens: bfloat16 [24576, 2048], P('sp'), may hold values from -6 to 6
- norm_gain: float32 [2048], replicated, may hold values from 0.1 to 1.9
- conv_value_w: bfloat16 [2048, 1024], P('sp', 'tp'), may hold values from -0.125 to 0.125
- conv_gate_w: bfloat16 [2048, 1024], P('sp', 'tp'), may hold values from -0.125 to 0.125
- query_w: bfloat16 [2048, 1024], P('sp', 'tp'), may hold values from -0.125 to 0.125
- key_w: bfloat16 [2048, 1024], P('sp', 'tp'), may hold values from -0.125 to 0.125
- value_w: bfloat16 [2048, 1024], P('sp', 'tp'), may hold values from -0.125 to 0.125
- out_gate_w: bfloat16 [2048, 1024], P('sp', 'tp'), may hold values from -0.125 to 0.125
- conv_out_w: bfloat16 [2048, 1024], P('sp', 'tp'), may hold values from -0.125 to 0.125
- ret_out_w: bfloat16 [2048, 1024], P('sp', 'tp'), may hold values from -0.125 to 0.125
- conv_taps: bfloat16 [31, 1024], replicated, may hold values from -3 to 3
- conv_gain: float32 [1024], replicated, may hold values from 0.1 to 1.9
- ret_gain: float32 [1024], replicated, may hold values from 0.1 to 1.9
- log_decay: float32 [8, 24576], P('tp', 'sp'), may hold values from -1 to 0, as said below
Outputs:
- mixed: bfloat16 [24576, 2048], P(('sp', 'tp'))
The draws below stay inside these ranges and needn't reach their ends.
Inputs may be any that keep to these rules, and one draw needn't show every extreme that they name: `log_decay`: every entry is at most zero.
All inputs are finite; a program needn't handle non-finite values.
Results may differ from the reference program's by a relative error of at most 0.03.
Values may be sent and summed in bfloat16 or wider, within the bound.
No kernel may reach another device: no remote copies, remote signals or barrier semaphores. Data moves between devices by JAX's collectives and lax.ppermute only.
A program may use at most 64 MiB of HBM per device.

```python
import math
import jax
import jax.numpy as jnp
from jax import lax

D = 2048
CONV_DIM = 1024
RET_HEADS = 8
HEAD_DIM = 128
CONV_WIDTH = 31
TOK_DEV = 192
RET_DIM = 1024
TOKEN_COUNT = 24576
N_SP = 128
N_TP = 4


def draw_log_decay(key, part):
    base_key = jax.random.fold_in(key, 17)
    order_key, fast_key, block_key, location_random_key, depth_key = jax.random.split(base_key, 5)
    ranking = jax.random.permutation(order_key, RET_HEADS)
    fast_head = ranking < RET_HEADS // 2
    fast_rate = -1.0 / jax.random.uniform(fast_key, (RET_HEADS,), jnp.float32, 30.0, 50.0)
    slow_rate = jnp.full((RET_HEADS,), -math.log(10.0) / (4.0 * TOKEN_COUNT), jnp.float32)
    head_decay_rate = jnp.where(fast_head, fast_rate, slow_rate)
    block_factor = jnp.exp(jax.random.uniform(block_key, (TOKEN_COUNT // TOK_DEV,), jnp.float32, -math.log(2.0), math.log(2.0)))
    position_scale_factor = jnp.repeat(block_factor, TOK_DEV, total_repeat_length=TOKEN_COUNT)
    spike_locations = jax.random.randint(location_random_key, (3,), 0, TOKEN_COUNT)
    layer_depths = jnp.log(jax.random.uniform(depth_key, (3,), jnp.float32, 0.5, 0.8))
    token_positions = jnp.arange(TOKEN_COUNT, dtype=jnp.int32)
    spike_values = jnp.sum(jnp.where(token_positions[:, None] == spike_locations[None, :], layer_depths[None, :], 0.0), axis=1)
    return (head_decay_rate[:, None] * position_scale_factor[None, :] + spike_values[None, :]).astype(jnp.float32)


def draw_conv_taps(key, part):
    base_key = jax.random.fold_in(key, 29)
    tap_noise = jnp.clip(jax.random.normal(base_key, (CONV_WIDTH, CONV_DIM), jnp.float32), -4.0, 4.0)
    rise_ratio = 5.0
    channel = jnp.arange(CONV_DIM, dtype=jnp.float32) / (CONV_DIM - 1)
    chan_scale = jnp.exp(math.log(rise_ratio) * (channel - 0.5))
    return (tap_noise * chan_scale[None, :] / math.sqrt(CONV_WIDTH)).astype(jnp.bfloat16)


def steps_of(key, dims, cuts, smallest, largest):
    factor_of = 1.0
    for dim, parts in cuts:
        steps = jax.random.uniform(jax.random.fold_in(jax.random.fold_in(key, 6), dim), (parts,), jnp.float32, smallest / len(cuts), largest / len(cuts))
        factor_of = factor_of * jnp.repeat(jnp.exp(steps), dims[dim] // parts).reshape((-1,) + (1,) * (len(dims) - 1 - dim))
    return factor_of


def gaussian(key, shape, deviation, reach, pieces=(), held_as=jnp.bfloat16):
    loudness = steps_of(key, shape, pieces, -0.22, 0.18) if pieces else 1.0
    entries = jax.random.normal(key, shape, jnp.float32) * deviation * loudness
    return jnp.minimum(jnp.maximum(entries, -reach), reach).astype(held_as)


def setup_inputs(seed: int = 0) -> dict:
    splits = jax.random.split(jax.random.key(seed), 15)
    return {
        "tokens": gaussian(splits[0], (TOKEN_COUNT, D), 1.0, 6.0, ((0, 128),)),
        "norm_gain": jnp.clip(1.0 + 0.18 * jax.random.normal(splits[1], (D,), jnp.float32), 0.1, 1.9),
        "conv_value_w": gaussian(splits[2], (D, CONV_DIM), D ** -0.5, 0.125, ((0, 128), (1, 4))),
        "conv_gate_w": gaussian(splits[3], (D, CONV_DIM), D ** -0.5, 0.125, ((0, 128), (1, 4))),
        "query_w": gaussian(splits[4], (D, RET_DIM), D ** -0.5, 0.125, ((0, 128), (1, 4))),
        "key_w": gaussian(splits[5], (D, RET_DIM), D ** -0.5, 0.125, ((0, 128), (1, 4))),
        "value_w": gaussian(splits[6], (D, RET_DIM), D ** -0.5, 0.125, ((0, 128), (1, 4))),
        "out_gate_w": gaussian(splits[7], (D, RET_DIM), D ** -0.5, 0.125, ((0, 128), (1, 4))),
        "conv_out_w": gaussian(splits[8], (D, CONV_DIM), (CONV_DIM + RET_DIM) ** -0.5, 0.125, ((0, 128), (1, 4))),
        "ret_out_w": gaussian(splits[9], (D, RET_DIM), (CONV_DIM + RET_DIM) ** -0.5, 0.125, ((0, 128), (1, 4))),
        "conv_taps": draw_conv_taps(jax.random.fold_in(splits[14], 71), 0),
        "conv_gain": jnp.clip(1.0 + 0.18 * jax.random.normal(splits[11], (CONV_DIM,), jnp.float32), 0.1, 1.9),
        "ret_gain": jnp.clip(1.0 + 0.18 * jax.random.normal(splits[12], (RET_DIM,), jnp.float32), 0.1, 1.9),
        "log_decay": draw_log_decay(jax.random.fold_in(splits[14], 71), 0),
    }


EPSILON = 1e-06
ROPE_BASE = 10000.0

def rotate(values, token_positions):
    half_dim = values.shape[-1] // 2
    frequency = ROPE_BASE ** (-jnp.arange(0, 2 * half_dim, 2, dtype=jnp.float32) / (2 * half_dim))
    angles = token_positions.astype(jnp.float32)[:, None] * frequency[None, :]
    cosine = jnp.cos(angles)[:, None, :]
    sine_part = jnp.sin(angles)[:, None, :]
    first_half = values[..., :half_dim]
    second = values[..., half_dim:]
    return jnp.concatenate([first_half * cosine - second * sine_part, first_half * sine_part + second * cosine], axis=-1)

def reference(tokens, norm_gain, conv_value_w, conv_gate_w, query_w, key_w, value_w, out_gate_w, conv_out_w, ret_out_w, conv_taps, conv_gain, ret_gain, log_decay):
    block_tokens = tokens.reshape(N_SP, TOK_DEV, D)
    block_decay = jnp.transpose(log_decay.reshape(RET_HEADS, N_SP, TOK_DEV), (1, 0, 2))
    block_index = jnp.arange(N_SP, dtype=jnp.int32)
    taps_float = conv_taps.astype(jnp.float32)
    conv_group = CONV_DIM // N_TP
    ret_group = RET_DIM // N_TP
    conv_out_float = conv_out_w.astype(jnp.float32).reshape(D, N_TP, conv_group)
    ret_out_float = ret_out_w.astype(jnp.float32).reshape(D, N_TP, ret_group)
    token_iota = jnp.arange(TOK_DEV, dtype=jnp.int32)
    later_mask = token_iota[:, None] >= token_iota[None, :]

    def one_block(carry, inputs):
        state, rim_rows = carry
        x_block, decay_block, index = inputs
        tok_float = x_block.astype(jnp.float32)
        normed = (tok_float * lax.rsqrt(lax.optimization_barrier(jnp.mean(tok_float * tok_float, axis=-1, keepdims=True)) + EPSILON) * norm_gain).astype(jnp.bfloat16)

        def project(weight):
            return jnp.dot(normed, weight, preferred_element_type=jnp.float32).astype(jnp.bfloat16)
        conv_value = project(conv_value_w)
        conv_gate = project(conv_gate_w)
        conv_gated = (conv_value.astype(jnp.float32) * jax.nn.sigmoid(conv_gate.astype(jnp.float32))).astype(jnp.bfloat16)
        padded = jnp.concatenate([rim_rows, conv_gated], axis=0)
        conv_sum = jnp.zeros((TOK_DEV, CONV_DIM), jnp.float32)
        for tap_index in range(CONV_WIDTH):
            conv_sum = conv_sum + padded[tap_index:tap_index + TOK_DEV].astype(jnp.float32) * taps_float[tap_index]
        chan_mean = lax.optimization_barrier(jnp.sum(conv_sum, axis=-1, keepdims=True)) / CONV_DIM
        chan_square = lax.optimization_barrier(jnp.sum(conv_sum * conv_sum, axis=-1, keepdims=True)) / CONV_DIM
        chan_var = chan_square - chan_mean * chan_mean
        conv_hidden = jax.nn.silu((conv_sum - chan_mean) * lax.rsqrt(chan_var + EPSILON) * conv_gain).astype(jnp.bfloat16)
        token_positions = index * TOK_DEV + token_iota
        query_rows = (rotate(project(query_w).astype(jnp.float32).reshape(TOK_DEV, RET_HEADS, HEAD_DIM), token_positions) * HEAD_DIM ** (-0.5)).astype(jnp.bfloat16)
        key_rows = rotate(project(key_w).astype(jnp.float32).reshape(TOK_DEV, RET_HEADS, HEAD_DIM), token_positions).astype(jnp.bfloat16)
        value_rows = project(value_w).reshape(TOK_DEV, RET_HEADS, HEAD_DIM)
        out_gate = project(out_gate_w)
        running = jnp.cumsum(decay_block, axis=1)
        log_gap = running[:, :, None] - running[:, None, :]
        decay_matrix = jnp.where(later_mask[None], jnp.exp(jnp.where(later_mask[None], log_gap, 0.0)), 0.0)
        scores = jnp.einsum('thd,shd->hts', query_rows.astype(jnp.float32), key_rows.astype(jnp.float32))
        weights_intra = (scores * decay_matrix).astype(jnp.bfloat16)
        intra_part = jnp.einsum('hts,shd->thd', weights_intra.astype(jnp.float32), value_rows.astype(jnp.float32))
        to_end = jnp.exp(running[:, -1:] - running)
        key_weighted = (key_rows.astype(jnp.float32) * jnp.transpose(to_end)[:, :, None]).astype(jnp.bfloat16)
        block_state = jnp.einsum('thd,the->hde', key_weighted.astype(jnp.float32), value_rows.astype(jnp.float32))
        cross_part = jnp.einsum('thd,hde->the', query_rows.astype(jnp.float32), state, precision=lax.Precision.HIGHEST) * jnp.transpose(jnp.exp(running))[:, :, None]
        merged = intra_part + cross_part
        new_state = state * jnp.exp(running[:, -1])[:, None, None] + block_state
        head_mean = lax.optimization_barrier(jnp.mean(merged, axis=-1, keepdims=True))
        head_var = lax.optimization_barrier(jnp.mean(jnp.square(merged - head_mean), axis=-1, keepdims=True))
        ret_norm = ((merged - head_mean) * lax.rsqrt(head_var + EPSILON)).reshape(TOK_DEV, RET_DIM) * ret_gain
        ret_hidden = (jax.nn.silu(out_gate.astype(jnp.float32)) * ret_norm).astype(jnp.bfloat16)
        conv_part = jnp.einsum('tgc,dgc->gtd', conv_hidden.astype(jnp.float32).reshape(TOK_DEV, N_TP, conv_group), conv_out_float)
        ret_part = jnp.einsum('tgc,dgc->gtd', ret_hidden.astype(jnp.float32).reshape(TOK_DEV, N_TP, ret_group), ret_out_float)
        partial_value = (conv_part + ret_part).astype(jnp.bfloat16)
        mixed = lax.optimization_barrier(jnp.sum(partial_value.astype(jnp.float32), axis=0)).astype(jnp.bfloat16)
        return ((new_state, conv_gated[TOK_DEV - CONV_WIDTH + 1:]), mixed)
    start_state = jnp.zeros((RET_HEADS, HEAD_DIM, HEAD_DIM), jnp.float32)
    start_rim = jnp.zeros((CONV_WIDTH - 1, CONV_DIM), jnp.bfloat16)
    final_carry, outputs = lax.scan(one_block, (start_state, start_rim), (block_tokens, block_decay, block_index))
    return outputs.reshape(TOKEN_COUNT, D)
```

```python
import jax
import jax.numpy as jnp
from jax import lax
from jax.experimental import pallas as pl
from jax.experimental.pallas import tpu as pltpu
from jax.sharding import Mesh
from jax.sharding import PartitionSpec as P

CONV_DIM = 1024
HEAD_DIM = 128
CONV_WIDTH = 31
HALO = 32
SP = ("sp_0", "sp_1", "sp_2")
SP_TP = ("sp_0", "sp_1", "sp_2", "tp")
EPSILON = 1e-06
ROPE_BASE = 10000.0
RING = 8
BF = jnp.bfloat16
F32 = jnp.float32


def place(z, y, core):
    return (z * RING + y) * 2 + core


def ring_groups(first):
    along_y = [[place(z, y, 0 if first else 1) for y in range(RING)] for z in range(RING)]
    along_z = [[place(z, y, 1 if first else 0) for z in range(RING)] for y in range(RING)]
    return along_y + along_z


def ring_step(step):
    pairs = []
    for z in range(RING):
        for y in range(RING):
            pairs.append((place(z, y, 0), place((z + step) % RING, y, 0)))
            pairs.append((place(z, y, 1), place(z, (y + step) % RING, 1)))
    return pairs


def told_to_all(x, axis, groups=None, count=RING):
    copies = jnp.broadcast_to(x[None], (count, *x.shape))
    return lax.all_to_all(copies, axis, 0, 0, axis_index_groups=groups, tiled=True)


def vmem(count):
    return [pl.BlockSpec(memory_space=pltpu.VMEM) for _ in range(count)]


def smem():
    return pl.BlockSpec(memory_space=pltpu.SMEM)


def call(body, outs, scalars, arrays, scratch=(), name=None):
    return pl.pallas_call(
        body,
        out_shape=outs,
        in_specs=[smem()] + vmem(len(arrays)),
        out_specs=vmem(len(outs)),
        scratch_shapes=list(scratch),
        compiler_params=pltpu.CompilerParams(vmem_limit_bytes=56 * 1024 * 1024),
        name=name,
    )(scalars, *arrays)


def like(shape, kind):
    return jax.ShapeDtypeStruct(shape, kind)


def prepare(where_ref, own_ref, partner_ref, halo_ref, gain_ref, normed_ref):
    core = where_ref[2]
    gain = gain_ref[...]

    def scaled(x):
        wide = x.astype(F32)
        mean = jnp.mean(wide * wide, axis=-1, keepdims=True)
        return (wide * lax.rsqrt(mean + EPSILON) * gain).astype(BF)

    rows = own_ref.shape[0]
    normed_ref[0:HALO, :] = scaled(halo_ref[...])
    for k in range(rows // 64):
        at = pl.multiple_of(HALO + core * rows + k * 64, 32)
        normed_ref[pl.ds(at, 64), :] = scaled(own_ref[k * 64 : (k + 1) * 64, :])
        at = pl.multiple_of(HALO + (1 - core) * rows + k * 64, 32)
        normed_ref[pl.ds(at, 64), :] = scaled(partner_ref[k * 64 : (k + 1) * 64, :])


def set_rows(target_ref, core, block, rows, first=0):
    height = rows.shape[0]

    @pl.when(core == 0)
    def _():
        target_ref[pl.ds(pl.multiple_of(block * 256 + first, 32), height), :] = rows

    @pl.when(core == 1)
    def _():
        for k in range(height // 32):
            at = pl.multiple_of((first // 32 + k) * 256 + block * 32, 32)
            target_ref[pl.ds(at, 32), :] = rows[k * 32 : (k + 1) * 32, :]


def rotated(raw, cosine, sine):
    half = pltpu.roll(raw, HEAD_DIM // 2, 1)
    return raw * cosine + half * sine


def key_value(where_ref, normed_ref, blocks_ref, cos_ref, sin_ref, end_ref, log_ref, key_ref, value_ref, sent_ref, w_ref):
    core = where_ref[2]
    for k in range(RING):
        set_rows(w_ref, core, k, blocks_ref[k])
    both = jnp.dot(normed_ref[HALO:, :], w_ref[...], preferred_element_type=F32)
    raw = both[:, :HEAD_DIM].astype(BF).astype(F32)
    value = both[:, HEAD_DIM:].astype(BF)
    key = rotated(raw, cos_ref[...], sin_ref[...]).astype(BF)
    key_ref[...] = key
    value_ref[...] = value
    weighted = (key.astype(F32) * end_ref[...]).astype(BF)
    state = lax.dot_general(weighted, value, (((0,), (0,)), ((), ())), preferred_element_type=F32)
    state = state.astype(BF)
    for k in range(RING):
        sent_ref[k, 0:HEAD_DIM, :] = state
        sent_ref[k, HEAD_DIM : HEAD_DIM + 16, :] = log_ref[...]


def log_of(ref, k):
    parts = ref[k, HEAD_DIM : HEAD_DIM + 16, :].astype(F32)
    return parts[0:1] + parts[1:2] + parts[2:3]


def in_parts(x):
    high = x.astype(BF)
    rest = x - high.astype(F32)
    middle = rest.astype(BF)
    low = (rest - middle.astype(F32)).astype(BF)
    return high, middle, low


def along_row(where_ref, got_ref, inside_ref, decay_ref, sent_ref):
    here = where_ref[1]
    before = jnp.zeros((1, HEAD_DIM), F32)
    whole = jnp.zeros((1, HEAD_DIM), F32)
    inside = jnp.zeros((HEAD_DIM, HEAD_DIM), F32)
    total = jnp.zeros((HEAD_DIM, HEAD_DIM), F32)
    for k in reversed(range(RING)):
        log = log_of(got_ref, k)
        state = got_ref[k, 0:HEAD_DIM, :].astype(F32)
        inside = inside + jnp.where(k < here, jnp.exp(before), 0.0) * state
        total = total + jnp.exp(whole) * state
        before = before + jnp.where(k < here, log, 0.0)
        whole = whole + log
    inside_ref[...] = inside
    decay_ref[...] = jnp.broadcast_to(jnp.exp(before), (8, HEAD_DIM))
    high, middle, low = in_parts(whole)
    row = lax.broadcasted_iota(jnp.int32, (16, HEAD_DIM), 0)
    logs = jnp.where(row == 0, high.astype(F32), jnp.where(row == 1, middle.astype(F32), jnp.where(row == 2, low.astype(F32), 0.0)))
    total = total.astype(BF)
    for k in range(RING):
        sent_ref[k, 0:HEAD_DIM, :] = total
        sent_ref[k, HEAD_DIM : HEAD_DIM + 16, :] = logs.astype(BF)


def conv_part(where_ref, normed_ref, taps_ref, r0, r1, r2, r3, r4, r5, r6, r7, r8, sums_ref, stats_ref, qg_ref, out_ref, cv_ref, gated_ref):
    core = where_ref[2]
    spot = jnp.where(core == 0, where_ref[0], where_ref[1])

    def put(ref, behind, first=0):
        block = lax.rem(spot - behind + RING, RING)
        for target, at in ((cv_ref, 0), (qg_ref, 256), (out_ref, 512)):
            set_rows(target, core, block, ref[:, at : at + 256], first)

    for behind, ref in enumerate((r0, r1, r2, r3)):
        put(ref, behind)
    put(r4, 4, 0)
    put(r5, 4, 128)
    for behind, ref in ((5, r6), (6, r7), (7, r8)):
        put(ref, behind)
    both = jnp.dot(normed_ref[...], cv_ref[...], preferred_element_type=F32)
    value = both[:, :HEAD_DIM].astype(BF).astype(F32)
    gate = both[:, HEAD_DIM:].astype(BF).astype(F32)
    gated_ref[...] = (value * jax.nn.sigmoid(gate)).astype(BF).astype(F32)
    rows = sums_ref.shape[0]
    lead = HALO - CONV_WIDTH + 1
    for at in range(0, rows, 64):
        total = jnp.zeros((64, HEAD_DIM), F32)
        for w in range(CONV_WIDTH):
            total = total + gated_ref[at + lead + w : at + lead + w + 64, :] * taps_ref[w : w + 1, :]
        sums_ref[at : at + 64, :] = total
    sums = sums_ref[...]
    ones = jnp.ones((8, HEAD_DIM), F32)
    over_lanes = (((1,), (1,)), ((), ()))
    first = lax.dot_general(ones, sums, over_lanes, precision=lax.Precision.HIGHEST, preferred_element_type=F32)
    second = lax.dot_general(ones, sums * sums, over_lanes, precision=lax.Precision.HIGHEST, preferred_element_type=F32)
    for k in range(8):
        stats_ref[k, 0:1, :] = first[0:1]
        stats_ref[k, 1:2, :] = second[0:1]


def inner_part(where_ref, normed_ref, qg_ref, cos_ref, sin_ref, key_ref, value_ref, col_ref, row_ref, query_ref, gate_ref, inner_ref):
    both = jnp.dot(normed_ref[HALO:, :], qg_ref[...], preferred_element_type=F32)
    raw = both[:, :HEAD_DIM].astype(BF).astype(F32)
    gate = both[:, HEAD_DIM:].astype(BF).astype(F32)
    query = (rotated(raw, cos_ref[...], sin_ref[...]) * HEAD_DIM ** (-0.5)).astype(BF)
    query_ref[...] = query
    gate_ref[...] = gate * jax.nn.sigmoid(gate)
    rows = query.shape[0]
    for at in range(0, rows, 128):
        upto = at + 128
        scores = lax.dot_general(query[at:upto], key_ref[0:upto, :], (((1,), (1,)), ((), ())), preferred_element_type=F32)
        mine = lax.broadcasted_iota(jnp.int32, scores.shape, 0) + at
        other = lax.broadcasted_iota(jnp.int32, scores.shape, 1)
        seen = mine >= other
        gap = col_ref[at:upto, :] - row_ref[:, 0:upto]
        decay = jnp.where(seen, jnp.exp(jnp.where(seen, gap, 0.0)), 0.0)
        weight = (scores * decay).astype(BF)
        inner_ref[at:upto, :] = jnp.dot(weight, value_ref[0:upto, :], preferred_element_type=F32)


def outer_part(where_ref, inner_ref, query_ref, gate_ref, col_ref, inside_ref, decay_ref, got_ref, gain_ref, sums_ref, stats_ref, conv_gain_ref, out_ref, keep_ref, send_ref, hidden_ref):
    core = where_ref[2]
    here = where_ref[0]
    before = jnp.zeros((1, HEAD_DIM), F32)
    rows_before = jnp.zeros((HEAD_DIM, HEAD_DIM), F32)
    for k in reversed(range(RING)):
        log = log_of(got_ref, k)
        state = got_ref[k, 0:HEAD_DIM, :].astype(F32)
        rows_before = rows_before + jnp.where(k < here, jnp.exp(before), 0.0) * state
        before = before + jnp.where(k < here, log, 0.0)
    state = inside_ref[...] + decay_ref[0:1, :] * rows_before
    cross = jnp.dot(query_ref[...].astype(F32), state, preferred_element_type=F32)
    merged = inner_ref[...] + cross * jnp.exp(col_ref[...])
    centred = merged - jnp.mean(merged, axis=-1, keepdims=True)
    spread = jnp.mean(centred * centred, axis=-1, keepdims=True)
    normed = centred * lax.rsqrt(spread + EPSILON) * gain_ref[...]
    hidden_ref[:, HEAD_DIM:] = (gate_ref[...] * normed).astype(BF)
    ones = jnp.ones((8, HEAD_DIM), F32)
    over_peers = (((0,), (0,)), ((), ()))
    firsts = jnp.concatenate([stats_ref[k, 0:1, :] for k in range(8)], axis=0)
    seconds = jnp.concatenate([stats_ref[k, 1:2, :] for k in range(8)], axis=0)
    mean = lax.dot_general(firsts, ones, over_peers, precision=lax.Precision.HIGHEST, preferred_element_type=F32) / CONV_DIM
    square = lax.dot_general(seconds, ones, over_peers, precision=lax.Precision.HIGHEST, preferred_element_type=F32) / CONV_DIM
    chan_var = square - mean * mean
    v = (sums_ref[...] - mean) * lax.rsqrt(chan_var + EPSILON) * conv_gain_ref[...]
    hidden_ref[:, :HEAD_DIM] = (v * jax.nn.sigmoid(v)).astype(BF)
    half = keep_ref.shape[0]
    mine = hidden_ref[pl.ds(pl.multiple_of(core * half, 64), half), :]
    theirs = hidden_ref[pl.ds(pl.multiple_of((1 - core) * half, 64), half), :]
    over_channels = (((1,), (1,)), ((), ()))
    send_ref[...] = lax.dot_general(theirs, out_ref[...], over_channels, preferred_element_type=F32).astype(BF)
    keep_ref[...] = lax.dot_general(mine, out_ref[...], over_channels, preferred_element_type=F32)


def rotary_tables(start, count):
    half = HEAD_DIM // 2
    frequency = ROPE_BASE ** (-jnp.arange(0, HEAD_DIM, 2, dtype=F32) / HEAD_DIM)
    positions = start + jnp.arange(count, dtype=jnp.int32)
    angles = positions.astype(F32)[:, None] * frequency[None, :]
    cosine, sine = jnp.cos(angles), jnp.sin(angles)
    del half
    return jnp.concatenate([cosine, cosine], axis=1), jnp.concatenate([-sine, sine], axis=1)


def per_device(
    tokens,
    norm_gain,
    conv_value_w,
    conv_gate_w,
    query_w,
    key_w,
    value_w,
    out_gate_w,
    conv_out_w,
    ret_out_w,
    conv_taps,
    conv_gain,
    ret_gain,
    log_decay,
):
    rows, width = tokens.shape
    both_rows = 2 * rows
    z, y, core, x = (lax.axis_index(a) for a in SP_TP)
    chip = z * RING + y
    where = jnp.stack([z, y, core]).astype(jnp.int32)

    parts = (key_w, value_w, conv_value_w, conv_gate_w, query_w, out_gate_w, conv_out_w, ret_out_w)
    for_cores = jnp.stack(
        [jnp.concatenate([w[:, h * HEAD_DIM : (h + 1) * HEAD_DIM] for w in parts], axis=1) for h in range(2)]
    )
    chip_rows = lax.all_to_all(for_cores, "sp_2", 0, 0, tiled=True).reshape(-1, 8 * HEAD_DIM)
    stage = told_to_all(chip_rows, SP, ring_groups(True)).reshape(-1, 8 * HEAD_DIM)

    swap = [(0, 1), (1, 0)]
    partner = lax.ppermute(tokens, "sp_2", swap)
    last = jnp.where(core == 1, tokens[rows - HALO :], partner[rows - HALO :])
    onward = [
        (k * 2 + c, (k + 1) * 2 + c) for k in range(RING * RING - 1) for c in range(2)
    ]
    halo = lax.ppermute(last, SP, onward)
    (normed,) = call(
        prepare,
        [like((HALO + both_rows, width), BF)],
        where,
        (tokens, partner, halo, norm_gain.reshape(1, width)),
        name="prepare",
    )

    decay = lax.all_to_all(log_decay, "sp_2", 0, 0, tiled=True).reshape(both_rows)
    running = jnp.cumsum(decay)
    to_end = jnp.exp(running[-1] - running).reshape(both_rows, 1)
    col = running.reshape(both_rows, 1)
    row = running.reshape(1, both_rows)
    logs = jnp.broadcast_to(jnp.stack(in_parts(running[-1]))[:, None], (3, HEAD_DIM))
    logs = jnp.pad(logs, ((0, 13), (0, 0)))
    cosine, sine = rotary_tables(chip * both_rows, both_rows)

    ahead, behind = ring_step(1), ring_step(-1)
    others = stage[:, 2 * HEAD_DIM :]
    f1, b1 = lax.ppermute(others, SP, ahead), lax.ppermute(others, SP, behind)
    kv = told_to_all(stage[:, : 2 * HEAD_DIM], SP, ring_groups(False))
    f2, b2 = lax.ppermute(f1, SP, ahead), lax.ppermute(b1, SP, behind)
    f3, b3 = lax.ppermute(f2, SP, ahead), lax.ppermute(b2, SP, behind)
    half = others.shape[0] // 2
    f4, b4 = lax.ppermute(f3[:half], SP, ahead), lax.ppermute(b3[half:], SP, behind)

    key, value, sent = call(
        key_value,
        [like((both_rows, HEAD_DIM), BF), like((both_rows, HEAD_DIM), BF), like((RING, HEAD_DIM + 16, HEAD_DIM), BF)],
        where,
        (normed, kv, cosine, sine, to_end, logs),
        [pltpu.VMEM((width, 2 * HEAD_DIM), BF)],
        name="key_value",
    )
    got = lax.all_to_all(sent, "sp_1", 0, 0, tiled=True)
    inside, decayed, sent = call(
        along_row,
        [like((HEAD_DIM, HEAD_DIM), F32), like((8, HEAD_DIM), F32), like((RING, HEAD_DIM + 16, HEAD_DIM), BF)],
        where,
        (got,),
        name="along_row",
    )
    got = lax.all_to_all(sent, "sp_0", 0, 0, tiled=True)

    channel = (x * 2 + core) * HEAD_DIM
    taps = lax.dynamic_slice_in_dim(conv_taps, channel, HEAD_DIM, 1).astype(F32)
    sums, stats, qg, out_w = call(
        conv_part,
        [
            like((both_rows, HEAD_DIM), F32),
            like((8, 2, both_rows), F32),
            like((width, 2 * HEAD_DIM), BF),
            like((width, 2 * HEAD_DIM), BF),
        ],
        where,
        (normed, taps, others, f1, f2, f3, f4, b4, b3, b2, b1),
        [pltpu.VMEM((width, 2 * HEAD_DIM), BF), pltpu.VMEM((HALO + both_rows, HEAD_DIM), F32)],
        name="conv_part",
    )
    stats = lax.all_to_all(stats, ("sp_2", "tp"), 0, 0, tiled=True)
    query, gate, inner = call(
        inner_part,
        [like((both_rows, HEAD_DIM), BF), like((both_rows, HEAD_DIM), F32), like((both_rows, HEAD_DIM), F32)],
        where,
        (normed, qg, cosine, sine, key, value, col, row),
        name="inner_part",
    )
    conv_gain_here = lax.dynamic_slice_in_dim(conv_gain, channel, HEAD_DIM, 0).reshape(1, HEAD_DIM)
    ret_gain_here = lax.dynamic_slice_in_dim(ret_gain, channel, HEAD_DIM, 0).reshape(1, HEAD_DIM)
    keep, send = call(
        outer_part,
        [like((rows, width), F32), like((rows, width), BF)],
        where,
        (inner, query, gate, col, inside, decayed, got, ret_gain_here, sums, stats, conv_gain_here, out_w),
        [pltpu.VMEM((both_rows, 2 * HEAD_DIM), BF)],
        name="outer_part",
    )
    other = lax.ppermute(send, "sp_2", swap)
    partial = (keep + other.astype(F32)).astype(BF)
    peers = lax.axis_size("tp")
    arrived = lax.all_to_all(partial.reshape(peers, rows // peers, width), "tp", 0, 0, tiled=True)
    return arrived.astype(F32).sum(axis=0).astype(BF)


def solution(mesh):
    finer = Mesh(mesh.devices.reshape(8, 8, 2, mesh.shape["tp"]), SP_TP)
    weight = P(SP, "tp")
    return jax.shard_map(
        per_device,
        mesh=finer,
        in_specs=(P(SP, None), P(), *[weight] * 8, P(), P(), P(), P("tp", SP)),
        out_specs=P(SP_TP, None),
        check_vma=False,
    )
```

```python
import jax
import jax.numpy as jnp
from jax import lax
from jax.experimental import pallas as pl
from jax.experimental.pallas import tpu as pltpu
from jax.sharding import Mesh
from jax.sharding import PartitionSpec as P

CONV_DIM = 1024
HEAD_DIM = 128
CONV_WIDTH = 31
HALO = 32
SP = ("sp_0", "sp_1", "sp_2")
SP_TP = ("sp_0", "sp_1", "sp_2", "tp")
EPSILON = 1e-06
ROPE_BASE = 10000.0
RING = 8
BF = jnp.bfloat16
F32 = jnp.float32

def place(z, y, core):
    return (z * RING + y) * 2 + core


def ring_groups(first):
    along_y = [[place(z, y, 0 if first else 1) for y in range(RING)] for z in range(RING)]
    along_z = [[place(z, y, 1 if first else 0) for z in range(RING)] for y in range(RING)]
    return along_y + along_z


def told_to_all(x, axis, groups=None, count=RING):
    copies = jnp.broadcast_to(x[None], (count, *x.shape))
    return lax.all_to_all(copies, axis, 0, 0, axis_index_groups=groups, tiled=True)


def vmem(count):
    return [pl.BlockSpec(memory_space=pltpu.VMEM) for _ in range(count)]


def smem():
    return pl.BlockSpec(memory_space=pltpu.SMEM)


def call(body, outs, scalars, arrays, scratch=(), name=None, far=0):
    return pl.pallas_call(
        body,
        out_shape=outs,
        in_specs=[smem()] + vmem(len(arrays) - far) + [pl.BlockSpec(memory_space=pl.ANY)] * far,
        out_specs=vmem(len(outs)),
        scratch_shapes=list(scratch),
        compiler_params=pltpu.CompilerParams(vmem_limit_bytes=56 * 1024 * 1024),
        name=name,
    )(scalars, *arrays)


def like(shape, kind):
    return jax.ShapeDtypeStruct(shape, kind)


def tall_dot(a, b, contract):
    return lax.dot_general(a, b, (contract, ((), ())), precision=lax.Precision.HIGHEST, preferred_element_type=F32)


def prepare(where_ref, own_ref, partner_ref, gain_ref, log_ref, other_log_ref, normed_ref, col_ref, row_ref):
    core = where_ref[2]
    gain = gain_ref[...]

    def scaled(x):
        wide = x.astype(F32)
        mean = jnp.mean(wide * wide, axis=-1, keepdims=True)
        return (wide * lax.rsqrt(mean + EPSILON) * gain).astype(BF)

    rows = own_ref.shape[0]
    for k in range(rows // 64):
        at = pl.multiple_of(core * rows + k * 64, 32)
        normed_ref[pl.ds(at, 64), :] = scaled(own_ref[k * 64 : (k + 1) * 64, :])
        at = pl.multiple_of((1 - core) * rows + k * 64, 32)
        normed_ref[pl.ds(at, 64), :] = scaled(partner_ref[k * 64 : (k + 1) * 64, :])
    own = jnp.where(core == 0, log_ref[0:1, :], log_ref[1:2, :])
    other = other_log_ref[...]
    upto = lax.broadcasted_iota(jnp.int32, (rows, rows), 0) >= lax.broadcasted_iota(jnp.int32, (rows, rows), 1)
    upto = jnp.where(upto, 1.0, 0.0)

    def summed(x):
        return tall_dot(upto, jnp.broadcast_to(x, (HEAD_DIM, rows)), ((1,), (1,)))

    first = summed(jnp.where(core == 0, own, other))
    second = summed(jnp.where(core == 0, other, own)) + first[rows - 1 : rows, :]
    col_ref[0:rows, :] = first
    col_ref[rows:, :] = second
    pick = jnp.where(lax.broadcasted_iota(jnp.int32, (8, HEAD_DIM), 1) == 0, 1.0, 0.0)
    row_ref[...] = tall_dot(pick, col_ref[...], ((1,), (1,)))


def assemble(*refs):
    weights, (out_ref, sem) = refs[:8], refs[8:]
    copies = []
    for h in range(2):
        for k, w_ref in enumerate(weights):
            source = w_ref.at[:, h * HEAD_DIM : (h + 1) * HEAD_DIM]
            target = out_ref.at[h, :, k * HEAD_DIM : (k + 1) * HEAD_DIM]
            copies.append(pltpu.make_async_copy(source, target, sem.at[h * 8 + k]))
    for c in copies:
        c.start()
    for c in copies:
        c.wait()


def set_rows(target_ref, core, block, rows, first=0):
    height = rows.shape[0]

    @pl.when(core == 0)
    def _():
        target_ref[pl.ds(pl.multiple_of(block * 256 + first, 32), height), :] = rows

    @pl.when(core == 1)
    def _():
        for k in range(height // 32):
            at = pl.multiple_of((first // 32 + k) * 256 + block * 32, 32)
            target_ref[pl.ds(at, 32), :] = rows[k * 32 : (k + 1) * 32, :]


def rotated(raw, cosine, sine):
    half = pltpu.roll(raw, HEAD_DIM // 2, 1)
    return raw * cosine + half * sine


def key_value(where_ref, normed_ref, blocks_ref, cos_ref, sin_ref, col_ref, key_ref, value_ref, sent_ref, w_ref):
    core = where_ref[2]
    for k in range(RING):
        set_rows(w_ref, core, k, blocks_ref[k])
    both = jnp.dot(normed_ref[...], w_ref[...], preferred_element_type=F32)
    raw = both[:, :HEAD_DIM].astype(BF).astype(F32)
    value = both[:, HEAD_DIM:].astype(BF)
    key = rotated(raw, cos_ref[...], sin_ref[...]).astype(BF)
    key_ref[...] = key
    value_ref[...] = value
    rows = key.shape[0]
    total = col_ref[rows - 1 : rows, :]
    weighted = (key.astype(F32) * jnp.exp(total - col_ref[...])).astype(BF)
    state = lax.dot_general(weighted, value, (((0,), (0,)), ((), ())), preferred_element_type=F32)
    send_state(sent_ref, state, total)


def send_state(sent_ref, state, log):
    high, middle, low = in_parts(log)
    row = lax.broadcasted_iota(jnp.int32, (16, HEAD_DIM), 0)
    logs = jnp.where(row == 0, high.astype(F32), jnp.where(row == 1, middle.astype(F32), jnp.where(row == 2, low.astype(F32), 0.0)))
    state, logs = state.astype(BF), logs.astype(BF)
    for k in range(RING):
        sent_ref[k, 0:HEAD_DIM, :] = state
        sent_ref[k, HEAD_DIM : HEAD_DIM + 16, :] = logs


def fetch(far_ref, part, near_ref, sem):
    return pltpu.make_async_copy(far_ref.at[:, part * 256 : (part + 1) * 256], near_ref, sem)


def in_order(target_ref, core, near_ref):
    for k in range(RING):
        set_rows(target_ref, core, k, near_ref[k * 256 : (k + 1) * 256, :])


def gated_part(where_ref, normed_ref, far_ref, gated_ref, near_ref, w_ref, sem):
    copy = fetch(far_ref, 0, near_ref, sem.at[0])
    copy.start()
    copy.wait()
    in_order(w_ref, where_ref[2], near_ref)
    both = jnp.dot(normed_ref[...], w_ref[...], preferred_element_type=F32)
    value = both[:, :HEAD_DIM].astype(BF).astype(F32)
    gate = both[:, HEAD_DIM:].astype(BF).astype(F32)
    gated_ref[...] = (value * jax.nn.sigmoid(gate)).astype(BF)


def log_of(ref, k):
    parts = ref[k, HEAD_DIM : HEAD_DIM + 16, :].astype(F32)
    return parts[0:1] + parts[1:2] + parts[2:3]


def in_parts(x):
    high = x.astype(BF)
    rest = x - high.astype(F32)
    middle = rest.astype(BF)
    low = (rest - middle.astype(F32)).astype(BF)
    return high, middle, low


def along_row(where_ref, got_ref, inside_ref, decay_ref, sent_ref):
    here = where_ref[1]
    before = jnp.zeros((1, HEAD_DIM), F32)
    whole = jnp.zeros((1, HEAD_DIM), F32)
    inside = jnp.zeros((HEAD_DIM, HEAD_DIM), F32)
    total = jnp.zeros((HEAD_DIM, HEAD_DIM), F32)
    for k in reversed(range(RING)):
        log = log_of(got_ref, k)
        state = got_ref[k, 0:HEAD_DIM, :].astype(F32)
        inside = inside + jnp.where(k < here, jnp.exp(before), 0.0) * state
        total = total + jnp.exp(whole) * state
        before = before + jnp.where(k < here, log, 0.0)
        whole = whole + log
    inside_ref[...] = inside
    decay_ref[...] = jnp.broadcast_to(jnp.exp(before), (8, HEAD_DIM))
    send_state(sent_ref, total, whole)


def conv_part(where_ref, own_ref, halo_ref, taps_ref, sums_ref, stats_ref, gated_ref):
    channel = pl.multiple_of((where_ref[3] * 2 + where_ref[2]) * HEAD_DIM, HEAD_DIM)
    gated_ref[0:HALO, :] = halo_ref[...].astype(F32)
    gated_ref[HALO:, :] = own_ref[...].astype(F32)
    taps = taps_ref[:, pl.ds(channel, HEAD_DIM)].astype(F32)
    rows = sums_ref.shape[0]
    lead = HALO - CONV_WIDTH + 1
    for at in range(0, rows, 64):
        total = jnp.zeros((64, HEAD_DIM), F32)
        for w in range(CONV_WIDTH):
            total = total + gated_ref[at + lead + w : at + lead + w + 64, :] * taps[w : w + 1, :]
        sums_ref[at : at + 64, :] = total
    sums = sums_ref[...]
    ones = jnp.ones((8, HEAD_DIM), F32)
    over_lanes = (((1,), (1,)), ((), ()))
    first = lax.dot_general(ones, sums, over_lanes, precision=lax.Precision.HIGHEST, preferred_element_type=F32)
    second = lax.dot_general(ones, sums * sums, over_lanes, precision=lax.Precision.HIGHEST, preferred_element_type=F32)
    for k in range(8):
        stats_ref[k, 0:1, :] = first[0:1]
        stats_ref[k, 1:2, :] = second[0:1]


def inner_part(where_ref, normed_ref, cos_ref, sin_ref, key_ref, value_ref, col_ref, row_ref, far_ref, query_ref, gate_ref, inner_ref, out_ref, near_ref, late_ref, qg_ref, sem):
    copies = [fetch(far_ref, 1, near_ref, sem.at[0]), fetch(far_ref, 2, late_ref, sem.at[1])]
    for c in copies:
        c.start()
    copies[0].wait()
    in_order(qg_ref, where_ref[2], near_ref)
    both = jnp.dot(normed_ref[...], qg_ref[...], preferred_element_type=F32)
    raw = both[:, :HEAD_DIM].astype(BF).astype(F32)
    gate = both[:, HEAD_DIM:].astype(BF).astype(F32)
    query = (rotated(raw, cos_ref[...], sin_ref[...]) * HEAD_DIM ** (-0.5)).astype(BF)
    query_ref[...] = query
    gate_ref[...] = gate * jax.nn.sigmoid(gate)
    rows = query.shape[0]
    for at in range(0, rows, 128):
        upto = at + 128
        scores = lax.dot_general(query[at:upto], key_ref[0:upto, :], (((1,), (1,)), ((), ())), preferred_element_type=F32)
        mine = lax.broadcasted_iota(jnp.int32, scores.shape, 0) + at
        other = lax.broadcasted_iota(jnp.int32, scores.shape, 1)
        seen = mine >= other
        gap = col_ref[at:upto, 0:1] - row_ref[0:1, 0:upto]
        decay = jnp.where(seen, jnp.exp(jnp.where(seen, gap, 0.0)), 0.0)
        weight = (scores * decay).astype(BF)
        inner_ref[at:upto, :] = jnp.dot(weight, value_ref[0:upto, :], preferred_element_type=F32)
    copies[1].wait()
    in_order(out_ref, where_ref[2], late_ref)


def outer_part(where_ref, inner_ref, query_ref, gate_ref, col_ref, inside_ref, decay_ref, got_ref, gain_ref, sums_ref, stats_ref, conv_gain_ref, out_ref, keep_ref, send_ref, hidden_ref):
    core = where_ref[2]
    here = where_ref[0]
    channel = pl.multiple_of((where_ref[3] * 2 + core) * HEAD_DIM, HEAD_DIM)
    before = jnp.zeros((1, HEAD_DIM), F32)
    rows_before = jnp.zeros((HEAD_DIM, HEAD_DIM), F32)
    for k in reversed(range(RING)):
        log = log_of(got_ref, k)
        state = got_ref[k, 0:HEAD_DIM, :].astype(F32)
        rows_before = rows_before + jnp.where(k < here, jnp.exp(before), 0.0) * state
        before = before + jnp.where(k < here, log, 0.0)
    state = inside_ref[...] + decay_ref[0:1, :] * rows_before
    cross = jnp.dot(query_ref[...].astype(F32), state, preferred_element_type=F32)
    merged = inner_ref[...] + cross * jnp.exp(col_ref[...])
    centred = merged - jnp.mean(merged, axis=-1, keepdims=True)
    spread = jnp.mean(centred * centred, axis=-1, keepdims=True)
    normed = centred * lax.rsqrt(spread + EPSILON) * gain_ref[:, pl.ds(channel, HEAD_DIM)]
    hidden_ref[:, HEAD_DIM:] = (gate_ref[...] * normed).astype(BF)
    ones = jnp.ones((8, HEAD_DIM), F32)
    over_peers = (((0,), (0,)), ((), ()))
    firsts = jnp.concatenate([stats_ref[k, 0:1, :] for k in range(8)], axis=0)
    seconds = jnp.concatenate([stats_ref[k, 1:2, :] for k in range(8)], axis=0)
    mean = lax.dot_general(firsts, ones, over_peers, precision=lax.Precision.HIGHEST, preferred_element_type=F32) / CONV_DIM
    square = lax.dot_general(seconds, ones, over_peers, precision=lax.Precision.HIGHEST, preferred_element_type=F32) / CONV_DIM
    chan_var = square - mean * mean
    v = (sums_ref[...] - mean) * lax.rsqrt(chan_var + EPSILON) * conv_gain_ref[:, pl.ds(channel, HEAD_DIM)]
    hidden_ref[:, :HEAD_DIM] = (v * jax.nn.sigmoid(v)).astype(BF)
    half = keep_ref.shape[0]
    mine = hidden_ref[pl.ds(pl.multiple_of(core * half, 64), half), :]
    theirs = hidden_ref[pl.ds(pl.multiple_of((1 - core) * half, 64), half), :]
    over_channels = (((1,), (1,)), ((), ()))
    send_ref[...] = lax.dot_general(theirs, out_ref[...], over_channels, preferred_element_type=F32).astype(BF)
    keep_ref[...] = lax.dot_general(mine, out_ref[...], over_channels, preferred_element_type=F32)


def rotary_tables(start, count):
    half = HEAD_DIM // 2
    frequency = ROPE_BASE ** (-jnp.arange(0, HEAD_DIM, 2, dtype=F32) / HEAD_DIM)
    positions = start + jnp.arange(count, dtype=jnp.int32)
    angles = positions.astype(F32)[:, None] * frequency[None, :]
    cosine, sine = jnp.cos(angles), jnp.sin(angles)
    del half
    return jnp.concatenate([cosine, cosine], axis=1), jnp.concatenate([-sine, sine], axis=1)


def per_device(
    tokens,
    norm_gain,
    conv_value_w,
    conv_gate_w,
    query_w,
    key_w,
    value_w,
    out_gate_w,
    conv_out_w,
    ret_out_w,
    conv_taps,
    conv_gain,
    ret_gain,
    log_decay,
):
    rows, width = tokens.shape
    both_rows = 2 * rows
    z, y, core, x = (lax.axis_index(a) for a in SP_TP)
    chip = z * RING + y
    where = jnp.stack([z, y, core, x]).astype(jnp.int32)

    parts = (key_w, value_w, conv_value_w, conv_gate_w, query_w, out_gate_w, conv_out_w, ret_out_w)
    for_cores = pl.pallas_call(
        assemble,
        out_shape=like((2, key_w.shape[0], 8 * HEAD_DIM), BF),
        in_specs=[pl.BlockSpec(memory_space=pl.ANY) for _ in parts],
        out_specs=pl.BlockSpec(memory_space=pltpu.VMEM),
        scratch_shapes=[pltpu.SemaphoreType.DMA((16,))],
        name="assemble",
    )(*parts)
    chip_rows = lax.all_to_all(for_cores, "sp_2", 0, 0, tiled=True).reshape(-1, 8 * HEAD_DIM)
    stage = told_to_all(chip_rows, SP, ring_groups(True)).reshape(-1, 8 * HEAD_DIM)

    swap = [(0, 1), (1, 0)]
    partner = lax.ppermute(tokens, "sp_2", swap)
    other_log = lax.ppermute(lax.dynamic_slice_in_dim(log_decay, 1 - core, 1, 0), "sp_2", swap)
    normed, col, row = call(
        prepare,
        [like((both_rows, width), BF), like((both_rows, HEAD_DIM), F32), like((8, both_rows), F32)],
        where,
        (tokens, partner, norm_gain.reshape(1, width), log_decay, other_log),
        name="prepare",
    )
    cosine, sine = rotary_tables(chip * both_rows, both_rows)
    stage, normed, col, row, cosine, sine = lax.optimization_barrier((stage, normed, col, row, cosine, sine))

    first = told_to_all(stage[:, : 2 * HEAD_DIM], SP, ring_groups(False))
    others = lax.all_gather(stage[:, 2 * HEAD_DIM :], SP, axis=0, axis_index_groups=ring_groups(False), tiled=True)

    key, value, sent = call(
        key_value,
        [like((both_rows, HEAD_DIM), BF), like((both_rows, HEAD_DIM), BF), like((RING, HEAD_DIM + 16, HEAD_DIM), BF)],
        where,
        (normed, first, cosine, sine, col),
        [pltpu.VMEM((width, 2 * HEAD_DIM), BF)],
        name="key_value",
    )
    got = lax.all_to_all(sent, "sp_1", 0, 0, tiled=True)
    inside, decayed, sent = call(
        along_row,
        [like((HEAD_DIM, HEAD_DIM), F32), like((8, HEAD_DIM), F32), like((RING, HEAD_DIM + 16, HEAD_DIM), BF)],
        where,
        (got,),
        name="along_row",
    )
    got = lax.all_to_all(sent, "sp_0", 0, 0, tiled=True)

    (gated,) = call(
        gated_part,
        [like((both_rows, HEAD_DIM), BF)],
        where,
        (normed, others),
        [pltpu.VMEM((width, 2 * HEAD_DIM), BF)] * 2 + [pltpu.SemaphoreType.DMA((1,))],
        name="gated_part",
        far=1,
    )
    onward = [(k * 2 + c, (k + 1) * 2 + c) for k in range(RING * RING - 1) for c in range(2)]
    halo = lax.ppermute(gated[both_rows - HALO :], SP, onward)
    sums, stats = call(
        conv_part,
        [like((both_rows, HEAD_DIM), F32), like((8, 2, both_rows), F32)],
        where,
        (gated, halo, conv_taps),
        [pltpu.VMEM((HALO + both_rows, HEAD_DIM), F32)],
        name="conv_part",
    )
    stats = lax.all_to_all(stats, ("sp_2", "tp"), 0, 0, tiled=True)
    query, gate, inner, out_w = call(
        inner_part,
        [
            like((both_rows, HEAD_DIM), BF),
            like((both_rows, HEAD_DIM), F32),
            like((both_rows, HEAD_DIM), F32),
            like((width, 2 * HEAD_DIM), BF),
        ],
        where,
        (normed, cosine, sine, key, value, col, row, others),
        [pltpu.VMEM((width, 2 * HEAD_DIM), BF)] * 3 + [pltpu.SemaphoreType.DMA((2,))],
        name="inner_part",
        far=1,
    )
    keep, send = call(
        outer_part,
        [like((rows, width), F32), like((rows, width), BF)],
        where,
        (inner, query, gate, col, inside, decayed, got, ret_gain.reshape(1, -1), sums, stats, conv_gain.reshape(1, -1), out_w),
        [pltpu.VMEM((both_rows, 2 * HEAD_DIM), BF)],
        name="outer_part",
    )
    other = lax.ppermute(send, "sp_2", swap)
    partial = (keep + other.astype(F32)).astype(BF)
    peers = lax.axis_size("tp")
    arrived = lax.all_to_all(partial.reshape(peers, rows // peers, width), "tp", 0, 0, tiled=True)
    return arrived.astype(F32).sum(axis=0).astype(BF)


def solution(mesh):
    finer = Mesh(mesh.devices.reshape(8, 8, 2, mesh.shape["tp"]), SP_TP)
    weight = P(SP, "tp")
    return jax.shard_map(
        per_device,
        mesh=finer,
        in_specs=(P(SP, None), P(), *[weight] * 8, P(), P(), P(), P("tp", SP)),
        out_specs=P(SP_TP, None),
        check_vma=False,
    )
```

```python
import jax
import jax.numpy as jnp
from jax import lax
from jax.experimental import pallas as pl
from jax.experimental.pallas import tpu as pltpu
from jax.sharding import Mesh
from jax.sharding import PartitionSpec as P


CONV_DIM = 1024
HEAD_DIM = 128
CONV_WIDTH = 31
HALO = 32
SP = ("sp_0", "sp_1", "sp_2")
SP_TP = ("sp_0", "sp_1", "sp_2", "tp")
EPSILON = 1e-06
ROPE_BASE = 10000.0
RING = 8
KV_MIB = 14
KV_FAR = ()
BF = jnp.bfloat16
F32 = jnp.float32


def place(z, y, core):
    return (z * RING + y) * 2 + core


def ring_groups(first):
    along_y = [[place(z, y, 0 if first else 1) for y in range(RING)] for z in range(RING)]
    along_z = [[place(z, y, 1 if first else 0) for z in range(RING)] for y in range(RING)]
    return along_y + along_z


def told_to_all(x, axis, groups=None, count=RING):
    copies = jnp.broadcast_to(x[None], (count, *x.shape))
    return lax.all_to_all(copies, axis, 0, 0, axis_index_groups=groups, tiled=True)


def call(body, outs, scalars, arrays, scratch=(), far=(), parts=(), far_outs=(), mib=56):
    n, m = len(arrays), len(outs)
    near = [pltpu.VMEM(arrays[i].shape, arrays[i].dtype) for i in far]
    near += [pltpu.VMEM((RING, 256, 256), BF) for _ in parts]
    near += [pltpu.VMEM(outs[i].shape, outs[i].dtype) for i in far_outs]
    scratch = list(scratch)

    def whole(where_ref, *refs):
        ins, rest = list(refs[:n]), refs[n:]
        results, rest = rest[:m], rest[m:]
        own, rest = rest[: len(scratch)], rest[len(scratch) :]
        results, sem = list(results), rest[-1] if near else None
        sources = [ins[i] for i in far] + [ins[i].at[:, p] for i, p in parts]
        copies = [pltpu.make_async_copy(a, rest[k], sem.at[k]) for k, a in enumerate(sources)]
        for c in copies:
            c.start()
        for c in copies:
            c.wait()
        for k, i in enumerate([*far, *(i for i, _ in parts)]):
            ins[i] = rest[k]
        copies = []
        for k, i in enumerate(far_outs, len(sources)):
            copies.append(pltpu.make_async_copy(rest[k], results[i], sem.at[k]))
            results[i] = rest[k]
        body(where_ref, *ins, *results, *own)
        for c in copies:
            c.start()
        for c in copies:
            c.wait()

    def spec(is_far):
        return pl.BlockSpec(memory_space=pltpu.HBM if is_far else pltpu.VMEM)

    sems = [pltpu.SemaphoreType.DMA((len(near),))] if near else []
    return pl.pallas_call(
        whole,
        out_shape=outs,
        in_specs=[pl.BlockSpec(memory_space=pltpu.SMEM)] + [spec(i in far or i in [j for j, _ in parts]) for i in range(n)],
        out_specs=[spec(i in far_outs) for i in range(m)],
        scratch_shapes=scratch + near + sems,
        compiler_params=pltpu.CompilerParams(vmem_limit_bytes=mib * 1024 * 1024),
    )(scalars, *arrays)


def like(shape, kind):
    return jax.ShapeDtypeStruct(shape, kind)


def tall_dot(a, b, contract):
    return lax.dot_general(a, b, (contract, ((), ())), precision=lax.Precision.HIGHEST, preferred_element_type=F32)


def scaled(x, gain):
    wide = x.astype(F32)
    mean = jnp.mean(wide * wide, axis=-1, keepdims=True)
    return (wide * lax.rsqrt(mean + EPSILON) * gain).astype(BF)


def prepare(where_ref, own_ref, partner_ref, gain_ref, normed_ref):
    core = where_ref[2]
    gain = gain_ref[...]
    rows = own_ref.shape[0]
    for k in range(rows // 64):
        at = pl.multiple_of(core * rows + k * 64, 32)
        normed_ref[pl.ds(at, 64), :] = scaled(own_ref[k * 64 : (k + 1) * 64, :], gain)
        at = pl.multiple_of((1 - core) * rows + k * 64, 32)
        normed_ref[pl.ds(at, 64), :] = scaled(partner_ref[k * 64 : (k + 1) * 64, :], gain)


def decays(where_ref, log_ref, other_log_ref, col_ref, row_ref):
    core = where_ref[2]
    rows = log_ref.shape[1]
    own = jnp.where(core == 0, log_ref[0:1, :], log_ref[1:2, :])
    other = other_log_ref[...]
    upto = lax.broadcasted_iota(jnp.int32, (rows, rows), 0) >= lax.broadcasted_iota(jnp.int32, (rows, rows), 1)
    upto = jnp.where(upto, 1.0, 0.0)

    def summed(x):
        return tall_dot(upto, jnp.broadcast_to(x, (HEAD_DIM, rows)), ((1,), (1,)))

    first = summed(jnp.where(core == 0, own, other))
    second = summed(jnp.where(core == 0, other, own)) + first[rows - 1 : rows, :]
    col_ref[0:rows, :] = first
    col_ref[rows:, :] = second
    pick = jnp.where(lax.broadcasted_iota(jnp.int32, (8, HEAD_DIM), 1) == 0, 1.0, 0.0)
    row_ref[...] = tall_dot(pick, col_ref[...], ((1,), (1,)))


def spread(mine_ref, theirs_ref, out_ref):
    core = lax.axis_index("sp_2")
    height = mine_ref.shape[0]
    at = pl.multiple_of(core * height, 16)
    other = pl.multiple_of((1 - core) * height, 16)
    mine, theirs = mine_ref[...], theirs_ref[...]
    for k in range(RING):
        out_ref[k, pl.ds(at, height), :] = mine
        out_ref[k, pl.ds(other, height), :] = theirs


def assemble(*refs):
    weights, (mine_ref, other_ref, sem) = refs[:8], refs[8:]
    core = lax.axis_index("sp_2")
    copies = []
    for h, out_ref in ((core, mine_ref), (1 - core, other_ref)):
        at = pl.multiple_of(h * HEAD_DIM, HEAD_DIM)
        for k, w_ref in enumerate(weights):
            target = out_ref.at[:, k * HEAD_DIM : (k + 1) * HEAD_DIM]
            copies.append(pltpu.make_async_copy(w_ref.at[:, pl.ds(at, HEAD_DIM)], target, sem.at[len(copies)]))
    for c in copies:
        c.start()
    for c in copies:
        c.wait()


def set_rows(target_ref, core, block, rows, first=0):
    height = rows.shape[0]

    @pl.when(core == 0)
    def _():
        target_ref[pl.ds(pl.multiple_of(block * 256 + first, 32), height), :] = rows

    @pl.when(core == 1)
    def _():
        for k in range(height // 32):
            at = pl.multiple_of((first // 32 + k) * 256 + block * 32, 32)
            target_ref[pl.ds(at, 32), :] = rows[k * 32 : (k + 1) * 32, :]


def rotated(raw, cosine, sine):
    half = pltpu.roll(raw, HEAD_DIM // 2, 1)
    return raw * cosine + half * sine


def key_value(where_ref, normed_ref, blocks_ref, cos_ref, sin_ref, col_ref, both_ref, sent_ref, w_ref):
    core = where_ref[2]
    for k in range(RING):
        set_rows(w_ref, core, k, blocks_ref[k])
    both = jnp.dot(normed_ref[...], w_ref[...], preferred_element_type=F32)
    raw = both[:, :HEAD_DIM].astype(BF).astype(F32)
    value = both[:, HEAD_DIM:].astype(BF)
    key = rotated(raw, cos_ref[...], sin_ref[...]).astype(BF)
    both_ref[:, :HEAD_DIM] = key
    both_ref[:, HEAD_DIM:] = value
    rows = key.shape[0]
    total = col_ref[rows - 1 : rows, :]
    weighted = (key.astype(F32) * jnp.exp(total - col_ref[...])).astype(BF)
    state = lax.dot_general(weighted, value, (((0,), (0,)), ((), ())), preferred_element_type=F32)
    send_state(sent_ref, state, total)


def send_state(sent_ref, state, log):
    high, middle, low = in_parts(log)
    row = lax.broadcasted_iota(jnp.int32, (16, HEAD_DIM), 0)
    logs = jnp.where(row == 0, high.astype(F32), jnp.where(row == 1, middle.astype(F32), jnp.where(row == 2, low.astype(F32), 0.0)))
    state, logs = state.astype(BF), logs.astype(BF)
    for k in range(RING):
        sent_ref[k, 0:HEAD_DIM, :] = state
        sent_ref[k, HEAD_DIM : HEAD_DIM + 16, :] = logs


def in_order(target_ref, core, near_ref):
    for k in range(RING):
        set_rows(target_ref, core, k, near_ref[k])


def log_of(ref, k):
    parts = ref[k, HEAD_DIM : HEAD_DIM + 16, :].astype(F32)
    return parts[0:1] + parts[1:2] + parts[2:3]


def in_parts(x):
    high = x.astype(BF)
    rest = x - high.astype(F32)
    middle = rest.astype(BF)
    low = (rest - middle.astype(F32)).astype(BF)
    return high, middle, low


def along_row(where_ref, got_ref, inside_ref, sent_ref):
    here = where_ref[1]
    before = jnp.zeros((1, HEAD_DIM), F32)
    whole = jnp.zeros((1, HEAD_DIM), F32)
    inside = jnp.zeros((HEAD_DIM, HEAD_DIM), F32)
    total = jnp.zeros((HEAD_DIM, HEAD_DIM), F32)
    for k in reversed(range(RING)):
        log = log_of(got_ref, k)
        state = got_ref[k, 0:HEAD_DIM, :].astype(F32)
        inside = inside + jnp.where(k < here, jnp.exp(before), 0.0) * state
        total = total + jnp.exp(whole) * state
        before = before + jnp.where(k < here, log, 0.0)
        whole = whole + log
    inside_ref[0:HEAD_DIM, :] = inside
    inside_ref[HEAD_DIM:, :] = jnp.broadcast_to(jnp.exp(before), (8, HEAD_DIM))
    send_state(sent_ref, total, whole)


def conv_part(where_ref, normed_ref, halo_ref, gain_ref, taps_ref, near_ref, sums_ref, stats_ref, w_ref, gated_ref):
    channel = pl.multiple_of((where_ref[3] * 2 + where_ref[2]) * HEAD_DIM, HEAD_DIM)
    in_order(w_ref, where_ref[2], near_ref)

    def gated(x):
        both = jnp.dot(x, w_ref[...], preferred_element_type=F32)
        value = both[:, :HEAD_DIM].astype(BF).astype(F32)
        gate = both[:, HEAD_DIM:].astype(BF).astype(F32)
        return (value * jax.nn.sigmoid(gate)).astype(BF).astype(F32)

    gated_ref[0:HALO, :] = gated(scaled(halo_ref[...], gain_ref[...]))
    gated_ref[HALO:, :] = gated(normed_ref[...])
    taps = taps_ref[:, pl.ds(channel, HEAD_DIM)].astype(F32)
    rows = sums_ref.shape[0]
    lead = HALO - CONV_WIDTH + 1
    for at in range(0, rows, 64):
        total = jnp.zeros((64, HEAD_DIM), F32)
        for w in range(CONV_WIDTH):
            total = total + gated_ref[at + lead + w : at + lead + w + 64, :] * taps[w : w + 1, :]
        sums_ref[at : at + 64, :] = total
    sums = sums_ref[...]
    ones = jnp.ones((8, HEAD_DIM), F32)
    over_lanes = (((1,), (1,)), ((), ()))
    first = lax.dot_general(ones, sums, over_lanes, precision=lax.Precision.HIGHEST, preferred_element_type=F32)
    second = lax.dot_general(ones, sums * sums, over_lanes, precision=lax.Precision.HIGHEST, preferred_element_type=F32)
    for k in range(8):
        stats_ref[k, 0:1, :] = first[0:1]
        stats_ref[k, 1:2, :] = second[0:1]


def inner_part(where_ref, normed_ref, cos_ref, sin_ref, key_value_ref, col_ref, row_ref, sums_ref, near_ref, packed_ref, qg_ref):
    in_order(qg_ref, where_ref[2], near_ref)
    both = jnp.dot(normed_ref[...], qg_ref[...], preferred_element_type=F32)
    raw = both[:, :HEAD_DIM].astype(BF).astype(F32)
    gate = both[:, HEAD_DIM:].astype(BF).astype(F32)
    query = (rotated(raw, cos_ref[...], sin_ref[...]) * HEAD_DIM ** (-0.5)).astype(BF)
    packed_ref[:, HEAD_DIM : 2 * HEAD_DIM] = query.astype(F32)
    packed_ref[:, 2 * HEAD_DIM : 3 * HEAD_DIM] = gate * jax.nn.sigmoid(gate)
    packed_ref[:, 3 * HEAD_DIM : 4 * HEAD_DIM] = jnp.exp(col_ref[...])
    packed_ref[:, 4 * HEAD_DIM :] = sums_ref[...]
    rows = query.shape[0]
    for at in range(0, rows, 128):
        upto = at + 128
        scores = lax.dot_general(query[at:upto], key_value_ref[0:upto, :HEAD_DIM], (((1,), (1,)), ((), ())), preferred_element_type=F32)
        mine = lax.broadcasted_iota(jnp.int32, scores.shape, 0) + at
        other = lax.broadcasted_iota(jnp.int32, scores.shape, 1)
        seen = mine >= other
        gap = col_ref[at:upto, 0:1] - row_ref[0:1, 0:upto]
        decay = jnp.where(seen, jnp.exp(jnp.where(seen, gap, 0.0)), 0.0)
        weight = (scores * decay).astype(BF)
        packed_ref[at:upto, :HEAD_DIM] = jnp.dot(weight, key_value_ref[0:upto, HEAD_DIM:], preferred_element_type=F32)


def outer_part(where_ref, packed_ref, inside_ref, got_ref, gain_ref, stats_ref, conv_gain_ref, blocks_ref, keep_ref, send_ref, hidden_ref, out_ref):
    core = where_ref[2]
    here = where_ref[0]
    channel = pl.multiple_of((where_ref[3] * 2 + core) * HEAD_DIM, HEAD_DIM)
    before = jnp.zeros((1, HEAD_DIM), F32)
    rows_before = jnp.zeros((HEAD_DIM, HEAD_DIM), F32)
    for k in reversed(range(RING)):
        log = log_of(got_ref, k)
        state = got_ref[k, 0:HEAD_DIM, :].astype(F32)
        rows_before = rows_before + jnp.where(k < here, jnp.exp(before), 0.0) * state
        before = before + jnp.where(k < here, log, 0.0)
    state = inside_ref[0:HEAD_DIM, :] + inside_ref[HEAD_DIM : HEAD_DIM + 1, :] * rows_before
    cross = jnp.dot(packed_ref[:, HEAD_DIM : 2 * HEAD_DIM], state, preferred_element_type=F32)
    merged = packed_ref[:, :HEAD_DIM] + cross * packed_ref[:, 3 * HEAD_DIM : 4 * HEAD_DIM]
    centred = merged - jnp.mean(merged, axis=-1, keepdims=True)
    spread = jnp.mean(centred * centred, axis=-1, keepdims=True)
    normed = centred * lax.rsqrt(spread + EPSILON) * gain_ref[:, pl.ds(channel, HEAD_DIM)]
    hidden_ref[:, HEAD_DIM:] = (packed_ref[:, 2 * HEAD_DIM : 3 * HEAD_DIM] * normed).astype(BF)
    ones = jnp.ones((8, HEAD_DIM), F32)
    over_peers = (((0,), (0,)), ((), ()))
    firsts = jnp.concatenate([stats_ref[k, 0:1, :] for k in range(8)], axis=0)
    seconds = jnp.concatenate([stats_ref[k, 1:2, :] for k in range(8)], axis=0)
    mean = lax.dot_general(firsts, ones, over_peers, precision=lax.Precision.HIGHEST, preferred_element_type=F32) / CONV_DIM
    square = lax.dot_general(seconds, ones, over_peers, precision=lax.Precision.HIGHEST, preferred_element_type=F32) / CONV_DIM
    chan_var = square - mean * mean
    v = (packed_ref[:, 4 * HEAD_DIM :] - mean) * lax.rsqrt(chan_var + EPSILON) * conv_gain_ref[:, pl.ds(channel, HEAD_DIM)]
    hidden_ref[:, :HEAD_DIM] = (v * jax.nn.sigmoid(v)).astype(BF)
    half = keep_ref.shape[0]
    for k in range(RING):
        set_rows(out_ref, core, k, blocks_ref[k, 2])
    mine = hidden_ref[pl.ds(pl.multiple_of(core * half, 64), half), :]
    theirs = hidden_ref[pl.ds(pl.multiple_of((1 - core) * half, 64), half), :]
    over_channels = (((1,), (1,)), ((), ()))
    send_ref[...] = lax.dot_general(theirs, out_ref[...], over_channels, preferred_element_type=F32).astype(BF)
    keep_ref[...] = lax.dot_general(mine, out_ref[...], over_channels, preferred_element_type=F32).astype(BF)


def rotary_tables(start, count):
    half = HEAD_DIM // 2
    frequency = ROPE_BASE ** (-jnp.arange(0, HEAD_DIM, 2, dtype=F32) / HEAD_DIM)
    positions = start + jnp.arange(count, dtype=jnp.int32)
    angles = positions.astype(F32)[:, None] * frequency[None, :]
    cosine, sine = jnp.cos(angles), jnp.sin(angles)
    del half
    return jnp.concatenate([cosine, cosine], axis=1), jnp.concatenate([-sine, sine], axis=1)


def per_device(
    tokens,
    norm_gain,
    conv_value_w,
    conv_gate_w,
    query_w,
    key_w,
    value_w,
    out_gate_w,
    conv_out_w,
    ret_out_w,
    conv_taps,
    conv_gain,
    ret_gain,
    log_decay,
):
    rows, width = tokens.shape
    both_rows = 2 * rows
    z, y, core, x = (lax.axis_index(a) for a in SP_TP)
    chip = z * RING + y
    where = jnp.stack([z, y, core, x]).astype(jnp.int32)

    parts = (key_w, value_w, conv_value_w, conv_gate_w, query_w, out_gate_w, conv_out_w, ret_out_w)
    half = like((key_w.shape[0], 8 * HEAD_DIM), BF)
    mine, other = pl.pallas_call(
        assemble,
        out_shape=[half, half],
        in_specs=[pl.BlockSpec(memory_space=pl.ANY) for _ in parts],
        out_specs=[pl.BlockSpec(memory_space=pltpu.VMEM)] * 2,
        scratch_shapes=[pltpu.SemaphoreType.DMA((16,))],
        compiler_params=pltpu.CompilerParams(vmem_limit_bytes=56 * 1024 * 1024),
        name="assemble",
    )(*parts)
    swap = [(0, 1), (1, 0)]
    theirs = lax.ppermute(other, "sp_2", swap)
    copies = pl.pallas_call(
        spread,
        out_shape=like((RING, 2 * key_w.shape[0], 8 * HEAD_DIM), BF),
        in_specs=[pl.BlockSpec(memory_space=pltpu.VMEM)] * 2,
        out_specs=pl.BlockSpec(memory_space=pltpu.VMEM),
        compiler_params=pltpu.CompilerParams(vmem_limit_bytes=4 * 1024 * 1024),
        name="spread",
    )(mine, theirs)
    stage = lax.all_to_all(copies, SP, 0, 0, axis_index_groups=ring_groups(True), tiled=True)
    stage = stage.reshape(-1, 8 * HEAD_DIM)

    partner = lax.ppermute(tokens, "sp_2", swap)
    other_log = lax.ppermute(lax.dynamic_slice_in_dim(log_decay, 1 - core, 1, 0), "sp_2", swap)
    (normed,) = call(
        prepare, [like((both_rows, width), BF)], where, (tokens, partner, norm_gain.reshape(1, width)), far=(0, 1)
    )
    stage, other_log, normed = lax.optimization_barrier((stage, other_log, normed))
    col, row = call(
        decays, [like((both_rows, HEAD_DIM), F32), like((8, both_rows), F32)], where, (log_decay, other_log), mib=8
    )
    cosine, sine = rotary_tables(chip * both_rows, both_rows)

    first = told_to_all(stage[:, : 2 * HEAD_DIM], SP, ring_groups(False))
    others = jnp.moveaxis(stage[:, 2 * HEAD_DIM :].reshape(-1, 3, 2 * HEAD_DIM), 1, 0)[None]
    others, col = lax.optimization_barrier((others, col))
    others = lax.all_gather(others, SP, axis=0, axis_index_groups=ring_groups(False), tiled=True)

    key_value_rows, sent = call(
        key_value,
        [like((both_rows, 2 * HEAD_DIM), BF), like((RING, HEAD_DIM + 16, HEAD_DIM), BF)],
        where,
        (normed, first, cosine, sine, col),
        [pltpu.VMEM((width, 2 * HEAD_DIM), BF)],
        mib=KV_MIB,
        far=KV_FAR,
    )
    last = jnp.where(core == 1, tokens[rows - HALO :], partner[rows - HALO :])
    last, _ = lax.optimization_barrier((last, sent))
    onward = [(k * 2 + c, (k + 1) * 2 + c) for k in range(RING * RING - 1) for c in range(2)]
    halo = lax.ppermute(last, SP, onward)
    got = lax.all_to_all(sent, "sp_1", 0, 0, tiled=True)
    got, halo = lax.optimization_barrier((got, halo))
    inside, sent = call(
        along_row,
        [like((HEAD_DIM + 8, HEAD_DIM), F32), like((RING, HEAD_DIM + 16, HEAD_DIM), BF)],
        where,
        (got,),
        mib=14,
    )
    got = lax.all_to_all(sent, "sp_0", 0, 0, tiled=True)

    sums, stats = call(
        conv_part,
        [like((both_rows, HEAD_DIM), F32), like((8, 2, both_rows), F32)],
        where,
        (normed, halo, norm_gain.reshape(1, width), conv_taps, others),
        [pltpu.VMEM((width, 2 * HEAD_DIM), BF), pltpu.VMEM((HALO + both_rows, HEAD_DIM), F32)],
        far=(0, 1, 2),
        parts=((4, 0),),
        far_outs=(0, 1),
    )
    (packed,) = call(
        inner_part,
        [like((both_rows, 5 * HEAD_DIM), F32)],
        where,
        (normed, cosine, sine, key_value_rows, col, row, sums, others),
        [pltpu.VMEM((width, 2 * HEAD_DIM), BF)],
        far=(0, 1, 2, 3, 4, 5, 6),
        parts=((7, 1),),
        far_outs=(0,),
    )
    stats, packed, got = lax.optimization_barrier((stats, packed, got))
    stats = lax.all_to_all(stats, ("sp_2", "tp"), 0, 0, tiled=True)
    keep, send = call(
        outer_part,
        [like((rows, width), BF), like((rows, width), BF)],
        where,
        (packed, inside, got, ret_gain.reshape(1, -1), stats, conv_gain.reshape(1, -1), others),
        [pltpu.VMEM((both_rows, 2 * HEAD_DIM), BF), pltpu.VMEM((width, 2 * HEAD_DIM), BF)],
        mib=14,
    )
    other = lax.ppermute(send, "sp_2", swap)
    partial = (keep.astype(F32) + other.astype(F32)).astype(BF)
    peers = lax.axis_size("tp")
    arrived = lax.all_to_all(partial.reshape(peers, rows // peers, width), "tp", 0, 0, tiled=True)
    return arrived.astype(F32).sum(axis=0).astype(BF)


def solution(mesh):
    finer = Mesh(mesh.devices.reshape(8, 8, 2, mesh.shape["tp"]), SP_TP)
    weight = P(SP, "tp")
    return jax.shard_map(
        per_device,
        mesh=finer,
        in_specs=(P(SP, None), P(), *[weight] * 8, P(), P(), P(), P("tp", SP)),
        out_specs=P(SP_TP, None),
        check_vma=False,
    )
```

```python
import jax
import jax.numpy as jnp
from jax import lax
from jax.experimental import pallas as pl
from jax.experimental.pallas import tpu as pltpu
from jax.sharding import Mesh
from jax.sharding import PartitionSpec as P


CONV_DIM = 1024
HEAD_DIM = 128
CONV_WIDTH = 31
HALO = 32
SP = ("sp_0", "sp_1", "sp_2")
SP_TP = ("sp_0", "sp_1", "sp_2", "tp")
EPSILON = 1e-06
ROPE_BASE = 10000.0
RING = 8
KV_MIB = 14
KV_FAR = ()
BF = jnp.bfloat16
F32 = jnp.float32


def place(z, y, core):
    return (z * RING + y) * 2 + core


def ring_groups(first):
    along_y = [[place(z, y, 0 if first else 1) for y in range(RING)] for z in range(RING)]
    along_z = [[place(z, y, 1 if first else 0) for z in range(RING)] for y in range(RING)]
    return along_y + along_z


def told_to_all(x, axis, groups=None, count=RING):
    copies = jnp.broadcast_to(x[None], (count, *x.shape))
    return lax.all_to_all(copies, axis, 0, 0, axis_index_groups=groups, tiled=True)


def call(body, outs, scalars, arrays, scratch=(), far=(), parts=(), far_outs=(), mib=56):
    n, m = len(arrays), len(outs)
    near = [pltpu.VMEM(arrays[i].shape, arrays[i].dtype) for i in far]
    near += [pltpu.VMEM((RING, 256, 256), BF) for _ in parts]
    near += [pltpu.VMEM(outs[i].shape, outs[i].dtype) for i in far_outs]
    scratch = list(scratch)

    def whole(where_ref, *refs):
        ins, rest = list(refs[:n]), refs[n:]
        results, rest = rest[:m], rest[m:]
        own, rest = rest[: len(scratch)], rest[len(scratch) :]
        results, sem = list(results), rest[-1] if near else None
        sources = [ins[i] for i in far] + [ins[i].at[:, p] for i, p in parts]
        copies = [pltpu.make_async_copy(a, rest[k], sem.at[k]) for k, a in enumerate(sources)]
        for c in copies:
            c.start()
        for c in copies:
            c.wait()
        for k, i in enumerate([*far, *(i for i, _ in parts)]):
            ins[i] = rest[k]
        copies = []
        for k, i in enumerate(far_outs, len(sources)):
            copies.append(pltpu.make_async_copy(rest[k], results[i], sem.at[k]))
            results[i] = rest[k]
        body(where_ref, *ins, *results, *own)
        for c in copies:
            c.start()
        for c in copies:
            c.wait()

    def spec(is_far):
        return pl.BlockSpec(memory_space=pltpu.HBM if is_far else pltpu.VMEM)

    sems = [pltpu.SemaphoreType.DMA((len(near),))] if near else []
    return pl.pallas_call(
        whole,
        out_shape=outs,
        in_specs=[pl.BlockSpec(memory_space=pltpu.SMEM)] + [spec(i in far or i in [j for j, _ in parts]) for i in range(n)],
        out_specs=[spec(i in far_outs) for i in range(m)],
        scratch_shapes=scratch + near + sems,
        compiler_params=pltpu.CompilerParams(vmem_limit_bytes=mib * 1024 * 1024),
    )(scalars, *arrays)


def like(shape, kind):
    return jax.ShapeDtypeStruct(shape, kind)


def tall_dot(a, b, contract):
    return lax.dot_general(a, b, (contract, ((), ())), precision=lax.Precision.HIGHEST, preferred_element_type=F32)


def scaled(x, gain):
    wide = x.astype(F32)
    mean = jnp.mean(wide * wide, axis=-1, keepdims=True)
    return (wide * lax.rsqrt(mean + EPSILON) * gain).astype(BF)


def prepare(where_ref, own_ref, partner_ref, gain_ref, normed_ref):
    core = where_ref[2]
    gain = gain_ref[...]
    rows = own_ref.shape[0]
    for k in range(rows // 64):
        at = pl.multiple_of(core * rows + k * 64, 32)
        normed_ref[pl.ds(at, 64), :] = scaled(own_ref[k * 64 : (k + 1) * 64, :], gain)
        at = pl.multiple_of((1 - core) * rows + k * 64, 32)
        normed_ref[pl.ds(at, 64), :] = scaled(partner_ref[k * 64 : (k + 1) * 64, :], gain)


def decays(where_ref, log_ref, other_log_ref, col_ref, row_ref):
    core = where_ref[2]
    rows = log_ref.shape[1]
    own = jnp.where(core == 0, log_ref[0:1, :], log_ref[1:2, :])
    other = other_log_ref[...]
    upto = lax.broadcasted_iota(jnp.int32, (rows, rows), 0) >= lax.broadcasted_iota(jnp.int32, (rows, rows), 1)
    upto = jnp.where(upto, 1.0, 0.0)

    def summed(x):
        return tall_dot(upto, jnp.broadcast_to(x, (HEAD_DIM, rows)), ((1,), (1,)))

    first = summed(jnp.where(core == 0, own, other))
    second = summed(jnp.where(core == 0, other, own)) + first[rows - 1 : rows, :]
    col_ref[0:rows, :] = first
    col_ref[rows:, :] = second
    pick = jnp.where(lax.broadcasted_iota(jnp.int32, (8, HEAD_DIM), 1) == 0, 1.0, 0.0)
    row_ref[...] = tall_dot(pick, col_ref[...], ((1,), (1,)))


def hold(in_ref, out_ref):
    out_ref[...] = in_ref[...]


def spread(mine_ref, theirs_ref, out_ref):
    core = lax.axis_index("sp_2")
    height = mine_ref.shape[0]
    at = pl.multiple_of(core * height, 16)
    other = pl.multiple_of((1 - core) * height, 16)
    mine, theirs = mine_ref[...], theirs_ref[...]
    for k in range(RING):
        out_ref[k, pl.ds(at, height), :] = mine
        out_ref[k, pl.ds(other, height), :] = theirs


def assemble(*refs):
    weights, (mine_ref, other_ref, sem) = refs[:8], refs[8:]
    core = lax.axis_index("sp_2")
    copies = []
    for h, out_ref in ((core, mine_ref), (1 - core, other_ref)):
        at = pl.multiple_of(h * HEAD_DIM, HEAD_DIM)
        for k, w_ref in enumerate(weights):
            target = out_ref.at[:, k * HEAD_DIM : (k + 1) * HEAD_DIM]
            copies.append(pltpu.make_async_copy(w_ref.at[:, pl.ds(at, HEAD_DIM)], target, sem.at[len(copies)]))
    for c in copies:
        c.start()
    for c in copies:
        c.wait()


def set_rows(target_ref, core, block, rows, first=0):
    height = rows.shape[0]

    @pl.when(core == 0)
    def _():
        target_ref[pl.ds(pl.multiple_of(block * 256 + first, 32), height), :] = rows

    @pl.when(core == 1)
    def _():
        for k in range(height // 32):
            at = pl.multiple_of((first // 32 + k) * 256 + block * 32, 32)
            target_ref[pl.ds(at, 32), :] = rows[k * 32 : (k + 1) * 32, :]


def rotated(raw, cosine, sine):
    half = pltpu.roll(raw, HEAD_DIM // 2, 1)
    return raw * cosine + half * sine


def key_value(where_ref, normed_ref, blocks_ref, cos_ref, sin_ref, col_ref, both_ref, sent_ref, w_ref):
    core = where_ref[2]
    for k in range(RING):
        set_rows(w_ref, core, k, blocks_ref[k])
    both = jnp.dot(normed_ref[...], w_ref[...], preferred_element_type=F32)
    raw = both[:, :HEAD_DIM].astype(BF).astype(F32)
    value = both[:, HEAD_DIM:].astype(BF)
    key = rotated(raw, cos_ref[...], sin_ref[...]).astype(BF)
    both_ref[:, :HEAD_DIM] = key
    both_ref[:, HEAD_DIM:] = value
    rows = key.shape[0]
    total = col_ref[rows - 1 : rows, :]
    weighted = (key.astype(F32) * jnp.exp(total - col_ref[...])).astype(BF)
    state = lax.dot_general(weighted, value, (((0,), (0,)), ((), ())), preferred_element_type=F32)
    send_state(sent_ref, state, total)


def send_state(sent_ref, state, log):
    high, middle, low = in_parts(log)
    row = lax.broadcasted_iota(jnp.int32, (16, HEAD_DIM), 0)
    logs = jnp.where(row == 0, high.astype(F32), jnp.where(row == 1, middle.astype(F32), jnp.where(row == 2, low.astype(F32), 0.0)))
    state, logs = state.astype(BF), logs.astype(BF)
    for k in range(RING):
        sent_ref[k, 0:HEAD_DIM, :] = state
        sent_ref[k, HEAD_DIM : HEAD_DIM + 16, :] = logs


def in_order(target_ref, core, near_ref):
    for k in range(RING):
        set_rows(target_ref, core, k, near_ref[k])


def log_of(ref, k):
    parts = ref[k, HEAD_DIM : HEAD_DIM + 16, :].astype(F32)
    return parts[0:1] + parts[1:2] + parts[2:3]


def in_parts(x):
    high = x.astype(BF)
    rest = x - high.astype(F32)
    middle = rest.astype(BF)
    low = (rest - middle.astype(F32)).astype(BF)
    return high, middle, low


def along_row(where_ref, got_ref, inside_ref, sent_ref):
    here = where_ref[1]
    before = jnp.zeros((1, HEAD_DIM), F32)
    whole = jnp.zeros((1, HEAD_DIM), F32)
    inside = jnp.zeros((HEAD_DIM, HEAD_DIM), F32)
    total = jnp.zeros((HEAD_DIM, HEAD_DIM), F32)
    for k in reversed(range(RING)):
        log = log_of(got_ref, k)
        state = got_ref[k, 0:HEAD_DIM, :].astype(F32)
        inside = inside + jnp.where(k < here, jnp.exp(before), 0.0) * state
        total = total + jnp.exp(whole) * state
        before = before + jnp.where(k < here, log, 0.0)
        whole = whole + log
    inside_ref[0:HEAD_DIM, :] = inside
    inside_ref[HEAD_DIM:, :] = jnp.broadcast_to(jnp.exp(before), (8, HEAD_DIM))
    send_state(sent_ref, total, whole)


def conv_part(where_ref, normed_ref, halo_ref, gain_ref, taps_ref, near_ref, sums_ref, stats_ref, w_ref, gated_ref):
    channel = pl.multiple_of((where_ref[3] * 2 + where_ref[2]) * HEAD_DIM, HEAD_DIM)
    in_order(w_ref, where_ref[2], near_ref)

    def gated(x):
        both = jnp.dot(x, w_ref[...], preferred_element_type=F32)
        value = both[:, :HEAD_DIM].astype(BF).astype(F32)
        gate = both[:, HEAD_DIM:].astype(BF).astype(F32)
        return (value * jax.nn.sigmoid(gate)).astype(BF).astype(F32)

    gated_ref[0:HALO, :] = gated(scaled(halo_ref[...], gain_ref[...]))
    gated_ref[HALO:, :] = gated(normed_ref[...])
    taps = taps_ref[:, pl.ds(channel, HEAD_DIM)].astype(F32)
    rows = sums_ref.shape[0]
    lead = HALO - CONV_WIDTH + 1
    for at in range(0, rows, 64):
        total = jnp.zeros((64, HEAD_DIM), F32)
        for w in range(CONV_WIDTH):
            total = total + gated_ref[at + lead + w : at + lead + w + 64, :] * taps[w : w + 1, :]
        sums_ref[at : at + 64, :] = total
    sums = sums_ref[...]
    ones = jnp.ones((8, HEAD_DIM), F32)
    over_lanes = (((1,), (1,)), ((), ()))
    first = lax.dot_general(ones, sums, over_lanes, precision=lax.Precision.HIGHEST, preferred_element_type=F32)
    second = lax.dot_general(ones, sums * sums, over_lanes, precision=lax.Precision.HIGHEST, preferred_element_type=F32)
    for k in range(8):
        stats_ref[k, 0:1, :] = first[0:1]
        stats_ref[k, 1:2, :] = second[0:1]


def inner_part(where_ref, normed_ref, cos_ref, sin_ref, key_value_ref, col_ref, row_ref, near_ref, packed_ref, qg_ref):
    in_order(qg_ref, where_ref[2], near_ref)
    both = jnp.dot(normed_ref[...], qg_ref[...], preferred_element_type=F32)
    raw = both[:, :HEAD_DIM].astype(BF).astype(F32)
    gate = both[:, HEAD_DIM:].astype(BF).astype(F32)
    query = (rotated(raw, cos_ref[...], sin_ref[...]) * HEAD_DIM ** (-0.5)).astype(BF)
    packed_ref[:, HEAD_DIM : 2 * HEAD_DIM] = query.astype(F32)
    packed_ref[:, 2 * HEAD_DIM : 3 * HEAD_DIM] = gate * jax.nn.sigmoid(gate)
    packed_ref[:, 3 * HEAD_DIM : 4 * HEAD_DIM] = jnp.exp(col_ref[...])
    rows = query.shape[0]
    for at in range(0, rows, 128):
        upto = at + 128
        scores = lax.dot_general(query[at:upto], key_value_ref[0:upto, :HEAD_DIM], (((1,), (1,)), ((), ())), preferred_element_type=F32)
        mine = lax.broadcasted_iota(jnp.int32, scores.shape, 0) + at
        other = lax.broadcasted_iota(jnp.int32, scores.shape, 1)
        seen = mine >= other
        gap = col_ref[at:upto, 0:1] - row_ref[0:1, 0:upto]
        decay = jnp.where(seen, jnp.exp(jnp.where(seen, gap, 0.0)), 0.0)
        weight = (scores * decay).astype(BF)
        packed_ref[at:upto, :HEAD_DIM] = jnp.dot(weight, key_value_ref[0:upto, HEAD_DIM:], preferred_element_type=F32)


def middle_part(where_ref, normed_ref, halo_ref, gain_ref, taps_ref, cos_ref, sin_ref, key_value_ref, col_ref, row_ref, near_ref, late_ref, stats_ref, packed_ref, w_ref, gated_ref, qg_ref):
    sums_ref = packed_ref.at[:, 4 * HEAD_DIM : 5 * HEAD_DIM]
    conv_part(where_ref, normed_ref, halo_ref, gain_ref, taps_ref, near_ref, sums_ref, stats_ref, w_ref, gated_ref)
    inner_part(where_ref, normed_ref, cos_ref, sin_ref, key_value_ref, col_ref, row_ref, late_ref, packed_ref, qg_ref)


def outer_part(where_ref, packed_ref, inside_ref, got_ref, gain_ref, stats_ref, conv_gain_ref, blocks_ref, keep_ref, send_ref, hidden_ref, out_ref):
    core = where_ref[2]
    here = where_ref[0]
    channel = pl.multiple_of((where_ref[3] * 2 + core) * HEAD_DIM, HEAD_DIM)
    before = jnp.zeros((1, HEAD_DIM), F32)
    rows_before = jnp.zeros((HEAD_DIM, HEAD_DIM), F32)
    for k in reversed(range(RING)):
        log = log_of(got_ref, k)
        state = got_ref[k, 0:HEAD_DIM, :].astype(F32)
        rows_before = rows_before + jnp.where(k < here, jnp.exp(before), 0.0) * state
        before = before + jnp.where(k < here, log, 0.0)
    state = inside_ref[0:HEAD_DIM, :] + inside_ref[HEAD_DIM : HEAD_DIM + 1, :] * rows_before
    cross = jnp.dot(packed_ref[:, HEAD_DIM : 2 * HEAD_DIM], state, preferred_element_type=F32)
    merged = packed_ref[:, :HEAD_DIM] + cross * packed_ref[:, 3 * HEAD_DIM : 4 * HEAD_DIM]
    centred = merged - jnp.mean(merged, axis=-1, keepdims=True)
    spread = jnp.mean(centred * centred, axis=-1, keepdims=True)
    normed = centred * lax.rsqrt(spread + EPSILON) * gain_ref[:, pl.ds(channel, HEAD_DIM)]
    hidden_ref[:, HEAD_DIM:] = (packed_ref[:, 2 * HEAD_DIM : 3 * HEAD_DIM] * normed).astype(BF)
    ones = jnp.ones((8, HEAD_DIM), F32)
    over_peers = (((0,), (0,)), ((), ()))
    firsts = jnp.concatenate([stats_ref[k, 0:1, :] for k in range(8)], axis=0)
    seconds = jnp.concatenate([stats_ref[k, 1:2, :] for k in range(8)], axis=0)
    mean = lax.dot_general(firsts, ones, over_peers, precision=lax.Precision.HIGHEST, preferred_element_type=F32) / CONV_DIM
    square = lax.dot_general(seconds, ones, over_peers, precision=lax.Precision.HIGHEST, preferred_element_type=F32) / CONV_DIM
    chan_var = square - mean * mean
    v = (packed_ref[:, 4 * HEAD_DIM :] - mean) * lax.rsqrt(chan_var + EPSILON) * conv_gain_ref[:, pl.ds(channel, HEAD_DIM)]
    hidden_ref[:, :HEAD_DIM] = (v * jax.nn.sigmoid(v)).astype(BF)
    half = keep_ref.shape[0]
    for k in range(RING):
        set_rows(out_ref, core, k, blocks_ref[k, 2])
    mine = hidden_ref[pl.ds(pl.multiple_of(core * half, 64), half), :]
    theirs = hidden_ref[pl.ds(pl.multiple_of((1 - core) * half, 64), half), :]
    over_channels = (((1,), (1,)), ((), ()))
    send_ref[...] = lax.dot_general(theirs, out_ref[...], over_channels, preferred_element_type=F32).astype(BF)
    keep_ref[...] = lax.dot_general(mine, out_ref[...], over_channels, preferred_element_type=F32).astype(BF)


def rotary_tables(start, count):
    half = HEAD_DIM // 2
    frequency = ROPE_BASE ** (-jnp.arange(0, HEAD_DIM, 2, dtype=F32) / HEAD_DIM)
    positions = start + jnp.arange(count, dtype=jnp.int32)
    angles = positions.astype(F32)[:, None] * frequency[None, :]
    cosine, sine = jnp.cos(angles), jnp.sin(angles)
    del half
    return jnp.concatenate([cosine, cosine], axis=1), jnp.concatenate([-sine, sine], axis=1)


def per_device(
    tokens,
    norm_gain,
    conv_value_w,
    conv_gate_w,
    query_w,
    key_w,
    value_w,
    out_gate_w,
    conv_out_w,
    ret_out_w,
    conv_taps,
    conv_gain,
    ret_gain,
    log_decay,
):
    rows, width = tokens.shape
    both_rows = 2 * rows
    z, y, core, x = (lax.axis_index(a) for a in SP_TP)
    chip = z * RING + y
    where = jnp.stack([z, y, core, x]).astype(jnp.int32)

    parts = (key_w, value_w, conv_value_w, conv_gate_w, query_w, out_gate_w, conv_out_w, ret_out_w)
    half = like((key_w.shape[0], 8 * HEAD_DIM), BF)
    own, other = pl.pallas_call(
        assemble,
        out_shape=[half, half],
        in_specs=[pl.BlockSpec(memory_space=pl.ANY) for _ in parts],
        out_specs=[pl.BlockSpec(memory_space=pltpu.VMEM)] * 2,
        scratch_shapes=[pltpu.SemaphoreType.DMA((16,))],
        compiler_params=pltpu.CompilerParams(vmem_limit_bytes=56 * 1024 * 1024),
        name="assemble",
    )(*parts)
    swap = [(0, 1), (1, 0)]
    theirs = lax.ppermute(other, "sp_2", swap)
    mine = pl.pallas_call(
        hold,
        out_shape=half,
        in_specs=[pl.BlockSpec(memory_space=pltpu.VMEM)],
        out_specs=pl.BlockSpec(memory_space=pltpu.VMEM),
        compiler_params=pltpu.CompilerParams(vmem_limit_bytes=4 * 1024 * 1024),
        name="hold",
    )
    mine = mine(own)
    copies = pl.pallas_call(
        spread,
        out_shape=like((RING, 2 * key_w.shape[0], 8 * HEAD_DIM), BF),
        in_specs=[pl.BlockSpec(memory_space=pltpu.VMEM)] * 2,
        out_specs=pl.BlockSpec(memory_space=pltpu.VMEM),
        compiler_params=pltpu.CompilerParams(vmem_limit_bytes=4 * 1024 * 1024),
        name="spread",
    )(mine, theirs)
    stage = lax.all_to_all(copies, SP, 0, 0, axis_index_groups=ring_groups(True), tiled=True)
    stage = stage.reshape(-1, 8 * HEAD_DIM)

    partner = lax.ppermute(tokens, "sp_2", swap)
    other_log = lax.ppermute(lax.dynamic_slice_in_dim(log_decay, 1 - core, 1, 0), "sp_2", swap)
    (normed,) = call(
        prepare, [like((both_rows, width), BF)], where, (tokens, partner, norm_gain.reshape(1, width)), far=(0, 1)
    )
    stage, other_log, normed = lax.optimization_barrier((stage, other_log, normed))
    col, row = call(
        decays, [like((both_rows, HEAD_DIM), F32), like((8, both_rows), F32)], where, (log_decay, other_log), mib=8
    )
    cosine, sine = rotary_tables(chip * both_rows, both_rows)

    first = told_to_all(stage[:, : 2 * HEAD_DIM], SP, ring_groups(False))
    others = jnp.moveaxis(stage[:, 2 * HEAD_DIM :].reshape(-1, 3, 2 * HEAD_DIM), 1, 0)[None]
    others, col = lax.optimization_barrier((others, col))
    others = lax.all_gather(others, SP, axis=0, axis_index_groups=ring_groups(False), tiled=True)

    key_value_rows, sent = call(
        key_value,
        [like((both_rows, 2 * HEAD_DIM), BF), like((RING, HEAD_DIM + 16, HEAD_DIM), BF)],
        where,
        (normed, first, cosine, sine, col),
        [pltpu.VMEM((width, 2 * HEAD_DIM), BF)],
        mib=KV_MIB,
        far=KV_FAR,
    )
    last = jnp.where(core == 1, tokens[rows - HALO :], partner[rows - HALO :])
    last, _ = lax.optimization_barrier((last, sent))
    onward = [(k * 2 + c, (k + 1) * 2 + c) for k in range(RING * RING - 1) for c in range(2)]
    halo = lax.ppermute(last, SP, onward)
    got = lax.all_to_all(sent, "sp_1", 0, 0, tiled=True)
    got, halo = lax.optimization_barrier((got, halo))
    inside, sent = call(
        along_row,
        [like((HEAD_DIM + 8, HEAD_DIM), F32), like((RING, HEAD_DIM + 16, HEAD_DIM), BF)],
        where,
        (got,),
        mib=14,
    )
    got = lax.all_to_all(sent, "sp_0", 0, 0, tiled=True)

    stats, packed = call(
        middle_part,
        [like((8, 2, both_rows), F32), like((both_rows, 5 * HEAD_DIM), F32)],
        where,
        (normed, halo, norm_gain.reshape(1, width), conv_taps, cosine, sine, key_value_rows, col, row, others, others),
        [
            pltpu.VMEM((width, 2 * HEAD_DIM), BF),
            pltpu.VMEM((HALO + both_rows, HEAD_DIM), F32),
            pltpu.VMEM((width, 2 * HEAD_DIM), BF),
        ],
        far=(0, 1, 2, 4, 5, 6, 7, 8),
        parts=((9, 0), (10, 1)),
        far_outs=(0, 1),
    )
    stats, packed, got = lax.optimization_barrier((stats, packed, got))
    stats = lax.all_to_all(stats, ("sp_2", "tp"), 0, 0, tiled=True)
    keep, send = call(
        outer_part,
        [like((rows, width), BF), like((rows, width), BF)],
        where,
        (packed, inside, got, ret_gain.reshape(1, -1), stats, conv_gain.reshape(1, -1), others),
        [pltpu.VMEM((both_rows, 2 * HEAD_DIM), BF), pltpu.VMEM((width, 2 * HEAD_DIM), BF)],
        mib=14,
    )
    other = lax.ppermute(send, "sp_2", swap)
    partial = (keep.astype(F32) + other.astype(F32)).astype(BF)
    peers = lax.axis_size("tp")
    arrived = lax.all_to_all(partial.reshape(peers, rows // peers, width), "tp", 0, 0, tiled=True)
    return arrived.astype(F32).sum(axis=0).astype(BF)


def solution(mesh):
    finer = Mesh(mesh.devices.reshape(8, 8, 2, mesh.shape["tp"]), SP_TP)
    weight = P(SP, "tp")
    return jax.shard_map(
        per_device,
        mesh=finer,
        in_specs=(P(SP, None), P(), *[weight] * 8, P(), P(), P(), P("tp", SP)),
        out_specs=P(SP_TP, None),
        check_vma=False,
    )
```

```python
import jax
import jax.numpy as jnp
from jax import lax
from jax.experimental import pallas as pl
from jax.experimental.pallas import tpu as pltpu
from jax.sharding import Mesh
from jax.sharding import PartitionSpec as P


CONV_DIM = 1024
HEAD_DIM = 128
CONV_WIDTH = 31
HALO = 32
SP = ("sp_0", "sp_1", "sp_2")
SP_TP = ("sp_0", "sp_1", "sp_2", "tp")
EPSILON = 1e-06
ROPE_BASE = 10000.0
RING = 8
KV_MIB = 14
KV_FAR = ()
BF = jnp.bfloat16
F32 = jnp.float32


def place(z, y, core):
    return (z * RING + y) * 2 + core


def ring_groups(first):
    along_y = [[place(z, y, 0 if first else 1) for y in range(RING)] for z in range(RING)]
    along_z = [[place(z, y, 1 if first else 0) for z in range(RING)] for y in range(RING)]
    return along_y + along_z


def told_to_all(x, axis, groups=None, count=RING):
    copies = jnp.broadcast_to(x[None], (count, *x.shape))
    return lax.all_to_all(copies, axis, 0, 0, axis_index_groups=groups, tiled=True)


def call(body, outs, scalars, arrays, scratch=(), far=(), parts=(), far_outs=(), mib=56):
    n, m = len(arrays), len(outs)
    near = [pltpu.VMEM(arrays[i].shape, arrays[i].dtype) for i in far]
    near += [pltpu.VMEM((RING, 256, 256), BF) for _ in parts]
    near += [pltpu.VMEM(outs[i].shape, outs[i].dtype) for i in far_outs]
    scratch = list(scratch)

    def whole(where_ref, *refs):
        ins, rest = list(refs[:n]), refs[n:]
        results, rest = rest[:m], rest[m:]
        own, rest = rest[: len(scratch)], rest[len(scratch) :]
        results, sem = list(results), rest[-1] if near else None
        sources = [ins[i] for i in far] + [ins[i].at[:, p] for i, p in parts]
        copies = [pltpu.make_async_copy(a, rest[k], sem.at[k]) for k, a in enumerate(sources)]
        for c in copies:
            c.start()
        for c in copies:
            c.wait()
        for k, i in enumerate([*far, *(i for i, _ in parts)]):
            ins[i] = rest[k]
        copies = []
        for k, i in enumerate(far_outs, len(sources)):
            copies.append(pltpu.make_async_copy(rest[k], results[i], sem.at[k]))
            results[i] = rest[k]
        body(where_ref, *ins, *results, *own)
        for c in copies:
            c.start()
        for c in copies:
            c.wait()

    def spec(is_far):
        return pl.BlockSpec(memory_space=pltpu.HBM if is_far else pltpu.VMEM)

    sems = [pltpu.SemaphoreType.DMA((len(near),))] if near else []
    return pl.pallas_call(
        whole,
        out_shape=outs,
        in_specs=[pl.BlockSpec(memory_space=pltpu.SMEM)] + [spec(i in far or i in [j for j, _ in parts]) for i in range(n)],
        out_specs=[spec(i in far_outs) for i in range(m)],
        scratch_shapes=scratch + near + sems,
        compiler_params=pltpu.CompilerParams(vmem_limit_bytes=mib * 1024 * 1024),
    )(scalars, *arrays)


def like(shape, kind):
    return jax.ShapeDtypeStruct(shape, kind)


def tall_dot(a, b, contract):
    return lax.dot_general(a, b, (contract, ((), ())), precision=lax.Precision.HIGHEST, preferred_element_type=F32)


def scaled(x, gain):
    wide = x.astype(F32)
    mean = jnp.mean(wide * wide, axis=-1, keepdims=True)
    return (wide * lax.rsqrt(mean + EPSILON) * gain).astype(BF)


def prepare(where_ref, own_ref, partner_ref, gain_ref, normed_ref):
    core = where_ref[2]
    gain = gain_ref[...]
    rows = own_ref.shape[0]
    for k in range(rows // 64):
        at = pl.multiple_of(core * rows + k * 64, 32)
        normed_ref[pl.ds(at, 64), :] = scaled(own_ref[k * 64 : (k + 1) * 64, :], gain)
        at = pl.multiple_of((1 - core) * rows + k * 64, 32)
        normed_ref[pl.ds(at, 64), :] = scaled(partner_ref[k * 64 : (k + 1) * 64, :], gain)


def decays(where_ref, log_ref, other_log_ref, col_ref, row_ref):
    core = where_ref[2]
    rows = log_ref.shape[1]
    own = jnp.where(core == 0, log_ref[0:1, :], log_ref[1:2, :])
    other = other_log_ref[...]
    upto = lax.broadcasted_iota(jnp.int32, (rows, rows), 0) >= lax.broadcasted_iota(jnp.int32, (rows, rows), 1)
    upto = jnp.where(upto, 1.0, 0.0)

    def summed(x):
        return tall_dot(upto, jnp.broadcast_to(x, (HEAD_DIM, rows)), ((1,), (1,)))

    first = summed(jnp.where(core == 0, own, other))
    second = summed(jnp.where(core == 0, other, own)) + first[rows - 1 : rows, :]
    col_ref[0:rows, :] = first
    col_ref[rows:, :] = second
    pick = jnp.where(lax.broadcasted_iota(jnp.int32, (8, HEAD_DIM), 1) == 0, 1.0, 0.0)
    row_ref[...] = tall_dot(pick, col_ref[...], ((1,), (1,)))


def hold(in_ref, out_ref):
    out_ref[...] = in_ref[...]


def spread(mine_ref, theirs_ref, out_ref):
    core = lax.axis_index("sp_2")
    height = mine_ref.shape[0]
    at = pl.multiple_of(core * height, 16)
    other = pl.multiple_of((1 - core) * height, 16)
    mine, theirs = mine_ref[...], theirs_ref[...]
    for k in range(RING):
        out_ref[k, pl.ds(at, height), :] = mine
        out_ref[k, pl.ds(other, height), :] = theirs


def assemble(*refs):
    weights, (mine_ref, other_ref, sem) = refs[:8], refs[8:]
    core = lax.axis_index("sp_2")
    copies = []
    for h, out_ref in ((core, mine_ref), (1 - core, other_ref)):
        at = pl.multiple_of(h * HEAD_DIM, HEAD_DIM)
        for k, w_ref in enumerate(weights):
            target = out_ref.at[:, k * HEAD_DIM : (k + 1) * HEAD_DIM]
            copies.append(pltpu.make_async_copy(w_ref.at[:, pl.ds(at, HEAD_DIM)], target, sem.at[len(copies)]))
    for c in copies:
        c.start()
    for c in copies:
        c.wait()


def set_rows(target_ref, core, block, rows, first=0):
    height = rows.shape[0]

    @pl.when(core == 0)
    def _():
        target_ref[pl.ds(pl.multiple_of(block * 256 + first, 32), height), :] = rows

    @pl.when(core == 1)
    def _():
        for k in range(height // 32):
            at = pl.multiple_of((first // 32 + k) * 256 + block * 32, 32)
            target_ref[pl.ds(at, 32), :] = rows[k * 32 : (k + 1) * 32, :]


def rotated(raw, cosine, sine):
    half = pltpu.roll(raw, HEAD_DIM // 2, 1)
    return raw * cosine + half * sine


def key_value(where_ref, normed_ref, blocks_ref, cos_ref, sin_ref, col_ref, both_ref, sent_ref, w_ref):
    core = where_ref[2]
    for k in range(RING):
        set_rows(w_ref, core, k, blocks_ref[k])
    both = jnp.dot(normed_ref[...], w_ref[...], preferred_element_type=F32)
    raw = both[:, :HEAD_DIM].astype(BF).astype(F32)
    value = both[:, HEAD_DIM:].astype(BF)
    key = rotated(raw, cos_ref[...], sin_ref[...]).astype(BF)
    both_ref[:, :HEAD_DIM] = key
    both_ref[:, HEAD_DIM:] = value
    rows = key.shape[0]
    total = col_ref[rows - 1 : rows, :]
    weighted = (key.astype(F32) * jnp.exp(total - col_ref[...])).astype(BF)
    state = lax.dot_general(weighted, value, (((0,), (0,)), ((), ())), preferred_element_type=F32)
    send_state(sent_ref, state, total)


def send_state(sent_ref, state, log):
    high, middle, low = in_parts(log)
    row = lax.broadcasted_iota(jnp.int32, (16, HEAD_DIM), 0)
    logs = jnp.where(row == 0, high.astype(F32), jnp.where(row == 1, middle.astype(F32), jnp.where(row == 2, low.astype(F32), 0.0)))
    state, logs = state.astype(BF), logs.astype(BF)
    for k in range(RING):
        sent_ref[k, 0:HEAD_DIM, :] = state
        sent_ref[k, HEAD_DIM : HEAD_DIM + 16, :] = logs


def in_order(target_ref, core, near_ref):
    for k in range(RING):
        set_rows(target_ref, core, k, near_ref[k])


def log_of(ref, k):
    parts = ref[k, HEAD_DIM : HEAD_DIM + 16, :].astype(F32)
    return parts[0:1] + parts[1:2] + parts[2:3]


def in_parts(x):
    high = x.astype(BF)
    rest = x - high.astype(F32)
    middle = rest.astype(BF)
    low = (rest - middle.astype(F32)).astype(BF)
    return high, middle, low


def along_row(where_ref, got_ref, inside_ref, sent_ref):
    here = where_ref[1]
    before = jnp.zeros((1, HEAD_DIM), F32)
    whole = jnp.zeros((1, HEAD_DIM), F32)
    inside = jnp.zeros((HEAD_DIM, HEAD_DIM), F32)
    total = jnp.zeros((HEAD_DIM, HEAD_DIM), F32)
    for k in reversed(range(RING)):
        log = log_of(got_ref, k)
        state = got_ref[k, 0:HEAD_DIM, :].astype(F32)
        inside = inside + jnp.where(k < here, jnp.exp(before), 0.0) * state
        total = total + jnp.exp(whole) * state
        before = before + jnp.where(k < here, log, 0.0)
        whole = whole + log
    inside_ref[0:HEAD_DIM, :] = inside
    inside_ref[HEAD_DIM:, :] = jnp.broadcast_to(jnp.exp(before), (8, HEAD_DIM))
    send_state(sent_ref, total, whole)


def conv_part(where_ref, normed_ref, halo_ref, gain_ref, taps_ref, near_ref, sums_ref, stats_ref, w_ref, gated_ref):
    channel = pl.multiple_of((where_ref[3] * 2 + where_ref[2]) * HEAD_DIM, HEAD_DIM)
    in_order(w_ref, where_ref[2], near_ref)

    def gated(x):
        both = jnp.dot(x, w_ref[...], preferred_element_type=F32)
        value = both[:, :HEAD_DIM].astype(BF).astype(F32)
        gate = both[:, HEAD_DIM:].astype(BF).astype(F32)
        return (value * jax.nn.sigmoid(gate)).astype(BF).astype(F32)

    gated_ref[0:HALO, :] = gated(scaled(halo_ref[...], gain_ref[...]))
    gated_ref[HALO:, :] = gated(normed_ref[...])
    taps = taps_ref[:, pl.ds(channel, HEAD_DIM)].astype(F32)
    rows = sums_ref.shape[0]
    lead = HALO - CONV_WIDTH + 1
    for at in range(0, rows, 64):
        total = jnp.zeros((64, HEAD_DIM), F32)
        for w in range(CONV_WIDTH):
            total = total + gated_ref[at + lead + w : at + lead + w + 64, :] * taps[w : w + 1, :]
        sums_ref[at : at + 64, :] = total
    sums = sums_ref[...]
    ones = jnp.ones((8, HEAD_DIM), F32)
    over_lanes = (((1,), (1,)), ((), ()))
    first = lax.dot_general(ones, sums, over_lanes, precision=lax.Precision.HIGHEST, preferred_element_type=F32)
    second = lax.dot_general(ones, sums * sums, over_lanes, precision=lax.Precision.HIGHEST, preferred_element_type=F32)
    for k in range(8):
        stats_ref[k, 0:1, :] = first[0:1]
        stats_ref[k, 1:2, :] = second[0:1]


def inner_part(where_ref, normed_ref, cos_ref, sin_ref, key_value_ref, col_ref, row_ref, near_ref, packed_ref, qg_ref):
    in_order(qg_ref, where_ref[2], near_ref)
    both = jnp.dot(normed_ref[...], qg_ref[...], preferred_element_type=F32)
    raw = both[:, :HEAD_DIM].astype(BF).astype(F32)
    gate = both[:, HEAD_DIM:].astype(BF).astype(F32)
    query = (rotated(raw, cos_ref[...], sin_ref[...]) * HEAD_DIM ** (-0.5)).astype(BF)
    packed_ref[:, HEAD_DIM : 2 * HEAD_DIM] = query.astype(F32)
    packed_ref[:, 2 * HEAD_DIM : 3 * HEAD_DIM] = gate * jax.nn.sigmoid(gate)
    packed_ref[:, 3 * HEAD_DIM : 4 * HEAD_DIM] = jnp.exp(col_ref[...])
    rows = query.shape[0]
    for at in range(0, rows, 128):
        upto = at + 128
        scores = lax.dot_general(query[at:upto], key_value_ref[0:upto, :HEAD_DIM], (((1,), (1,)), ((), ())), preferred_element_type=F32)
        mine = lax.broadcasted_iota(jnp.int32, scores.shape, 0) + at
        other = lax.broadcasted_iota(jnp.int32, scores.shape, 1)
        seen = mine >= other
        gap = col_ref[at:upto, 0:1] - row_ref[0:1, 0:upto]
        decay = jnp.where(seen, jnp.exp(jnp.where(seen, gap, 0.0)), 0.0)
        weight = (scores * decay).astype(BF)
        packed_ref[at:upto, :HEAD_DIM] = jnp.dot(weight, key_value_ref[0:upto, HEAD_DIM:], preferred_element_type=F32)


def middle_part(where_ref, normed_ref, halo_ref, gain_ref, taps_ref, cos_ref, sin_ref, key_value_ref, col_ref, row_ref, near_ref, late_ref, stats_ref, packed_ref, w_ref, gated_ref, qg_ref):
    sums_ref = packed_ref.at[:, 4 * HEAD_DIM : 5 * HEAD_DIM]
    conv_part(where_ref, normed_ref, halo_ref, gain_ref, taps_ref, near_ref, sums_ref, stats_ref, w_ref, gated_ref)
    inner_part(where_ref, normed_ref, cos_ref, sin_ref, key_value_ref, col_ref, row_ref, late_ref, packed_ref, qg_ref)


def outer_part(where_ref, packed_ref, inside_ref, got_ref, gain_ref, stats_ref, conv_gain_ref, blocks_ref, send_ref, own_ref, out_ref, hidden_ref):
    core = where_ref[2]
    here = where_ref[0]
    channel = pl.multiple_of((where_ref[3] * 2 + core) * HEAD_DIM, HEAD_DIM)
    before = jnp.zeros((1, HEAD_DIM), F32)
    rows_before = jnp.zeros((HEAD_DIM, HEAD_DIM), F32)
    for k in reversed(range(RING)):
        log = log_of(got_ref, k)
        state = got_ref[k, 0:HEAD_DIM, :].astype(F32)
        rows_before = rows_before + jnp.where(k < here, jnp.exp(before), 0.0) * state
        before = before + jnp.where(k < here, log, 0.0)
    state = inside_ref[0:HEAD_DIM, :] + inside_ref[HEAD_DIM : HEAD_DIM + 1, :] * rows_before
    cross = jnp.dot(packed_ref[:, HEAD_DIM : 2 * HEAD_DIM], state, preferred_element_type=F32)
    merged = packed_ref[:, :HEAD_DIM] + cross * packed_ref[:, 3 * HEAD_DIM : 4 * HEAD_DIM]
    centred = merged - jnp.mean(merged, axis=-1, keepdims=True)
    spread = jnp.mean(centred * centred, axis=-1, keepdims=True)
    normed = centred * lax.rsqrt(spread + EPSILON) * gain_ref[:, pl.ds(channel, HEAD_DIM)]
    hidden_ref[:, HEAD_DIM:] = (packed_ref[:, 2 * HEAD_DIM : 3 * HEAD_DIM] * normed).astype(BF)
    ones = jnp.ones((8, HEAD_DIM), F32)
    over_peers = (((0,), (0,)), ((), ()))
    firsts = jnp.concatenate([stats_ref[k, 0:1, :] for k in range(8)], axis=0)
    seconds = jnp.concatenate([stats_ref[k, 1:2, :] for k in range(8)], axis=0)
    mean = lax.dot_general(firsts, ones, over_peers, precision=lax.Precision.HIGHEST, preferred_element_type=F32) / CONV_DIM
    square = lax.dot_general(seconds, ones, over_peers, precision=lax.Precision.HIGHEST, preferred_element_type=F32) / CONV_DIM
    chan_var = square - mean * mean
    v = (packed_ref[:, 4 * HEAD_DIM :] - mean) * lax.rsqrt(chan_var + EPSILON) * conv_gain_ref[:, pl.ds(channel, HEAD_DIM)]
    hidden_ref[:, :HEAD_DIM] = (v * jax.nn.sigmoid(v)).astype(BF)
    half = send_ref.shape[0]
    for k in range(RING):
        set_rows(out_ref, core, k, blocks_ref[k, 2])
    mine = hidden_ref[pl.ds(pl.multiple_of(core * half, 64), half), :]
    theirs = hidden_ref[pl.ds(pl.multiple_of((1 - core) * half, 64), half), :]
    over_channels = (((1,), (1,)), ((), ()))
    send_ref[...] = lax.dot_general(theirs, out_ref[...], over_channels, preferred_element_type=F32).astype(BF)
    own_ref[...] = mine


def keep_part(own_ref, out_ref, keep_ref):
    over_channels = (((1,), (1,)), ((), ()))
    keep_ref[...] = lax.dot_general(own_ref[...], out_ref[...], over_channels, preferred_element_type=F32).astype(BF)


def rotary_tables(start, count):
    half = HEAD_DIM // 2
    frequency = ROPE_BASE ** (-jnp.arange(0, HEAD_DIM, 2, dtype=F32) / HEAD_DIM)
    positions = start + jnp.arange(count, dtype=jnp.int32)
    angles = positions.astype(F32)[:, None] * frequency[None, :]
    cosine, sine = jnp.cos(angles), jnp.sin(angles)
    del half
    return jnp.concatenate([cosine, cosine], axis=1), jnp.concatenate([-sine, sine], axis=1)


def per_device(
    tokens,
    norm_gain,
    conv_value_w,
    conv_gate_w,
    query_w,
    key_w,
    value_w,
    out_gate_w,
    conv_out_w,
    ret_out_w,
    conv_taps,
    conv_gain,
    ret_gain,
    log_decay,
):
    rows, width = tokens.shape
    both_rows = 2 * rows
    z, y, core, x = (lax.axis_index(a) for a in SP_TP)
    chip = z * RING + y
    where = jnp.stack([z, y, core, x]).astype(jnp.int32)

    parts = (key_w, value_w, conv_value_w, conv_gate_w, query_w, out_gate_w, conv_out_w, ret_out_w)
    half = like((key_w.shape[0], 8 * HEAD_DIM), BF)
    own, other = pl.pallas_call(
        assemble,
        out_shape=[half, half],
        in_specs=[pl.BlockSpec(memory_space=pl.ANY) for _ in parts],
        out_specs=[pl.BlockSpec(memory_space=pltpu.VMEM)] * 2,
        scratch_shapes=[pltpu.SemaphoreType.DMA((16,))],
        compiler_params=pltpu.CompilerParams(vmem_limit_bytes=56 * 1024 * 1024),
        name="assemble",
    )(*parts)
    swap = [(0, 1), (1, 0)]
    theirs = lax.ppermute(other, "sp_2", swap)
    mine = pl.pallas_call(
        hold,
        out_shape=half,
        in_specs=[pl.BlockSpec(memory_space=pltpu.VMEM)],
        out_specs=pl.BlockSpec(memory_space=pltpu.VMEM),
        compiler_params=pltpu.CompilerParams(vmem_limit_bytes=4 * 1024 * 1024),
        name="hold",
    )
    mine = mine(own)
    copies = pl.pallas_call(
        spread,
        out_shape=like((RING, 2 * key_w.shape[0], 8 * HEAD_DIM), BF),
        in_specs=[pl.BlockSpec(memory_space=pltpu.VMEM)] * 2,
        out_specs=pl.BlockSpec(memory_space=pltpu.VMEM),
        compiler_params=pltpu.CompilerParams(vmem_limit_bytes=4 * 1024 * 1024),
        name="spread",
    )(mine, theirs)
    stage = lax.all_to_all(copies, SP, 0, 0, axis_index_groups=ring_groups(True), tiled=True)
    stage = stage.reshape(-1, 8 * HEAD_DIM)

    partner = lax.ppermute(tokens, "sp_2", swap)
    other_log = lax.ppermute(lax.dynamic_slice_in_dim(log_decay, 1 - core, 1, 0), "sp_2", swap)
    (normed,) = call(
        prepare, [like((both_rows, width), BF)], where, (tokens, partner, norm_gain.reshape(1, width)), far=(0, 1)
    )
    stage, other_log, normed = lax.optimization_barrier((stage, other_log, normed))
    col, row = call(
        decays, [like((both_rows, HEAD_DIM), F32), like((8, both_rows), F32)], where, (log_decay, other_log), mib=8
    )
    cosine, sine = rotary_tables(chip * both_rows, both_rows)

    first = told_to_all(stage[:, : 2 * HEAD_DIM], SP, ring_groups(False))
    others = jnp.moveaxis(stage[:, 2 * HEAD_DIM :].reshape(-1, 3, 2 * HEAD_DIM), 1, 0)[None]
    others, col = lax.optimization_barrier((others, col))
    others = lax.all_gather(others, SP, axis=0, axis_index_groups=ring_groups(False), tiled=True)

    key_value_rows, sent = call(
        key_value,
        [like((both_rows, 2 * HEAD_DIM), BF), like((RING, HEAD_DIM + 16, HEAD_DIM), BF)],
        where,
        (normed, first, cosine, sine, col),
        [pltpu.VMEM((width, 2 * HEAD_DIM), BF)],
        mib=KV_MIB,
        far=KV_FAR,
    )
    last = jnp.where(core == 1, tokens[rows - HALO :], partner[rows - HALO :])
    last, _ = lax.optimization_barrier((last, sent))
    onward = [(k * 2 + c, (k + 1) * 2 + c) for k in range(RING * RING - 1) for c in range(2)]
    halo = lax.ppermute(last, SP, onward)
    got = lax.all_to_all(sent, "sp_1", 0, 0, tiled=True)
    got, halo = lax.optimization_barrier((got, halo))
    inside, sent = call(
        along_row,
        [like((HEAD_DIM + 8, HEAD_DIM), F32), like((RING, HEAD_DIM + 16, HEAD_DIM), BF)],
        where,
        (got,),
        mib=14,
    )
    got = lax.all_to_all(sent, "sp_0", 0, 0, tiled=True)

    stats, packed = call(
        middle_part,
        [like((8, 2, both_rows), F32), like((both_rows, 5 * HEAD_DIM), F32)],
        where,
        (normed, halo, norm_gain.reshape(1, width), conv_taps, cosine, sine, key_value_rows, col, row, others, others),
        [
            pltpu.VMEM((width, 2 * HEAD_DIM), BF),
            pltpu.VMEM((HALO + both_rows, HEAD_DIM), F32),
            pltpu.VMEM((width, 2 * HEAD_DIM), BF),
        ],
        far=(0, 1, 2, 4, 5, 6, 7, 8),
        parts=((9, 0), (10, 1)),
        far_outs=(0, 1),
    )
    stats, packed, got = lax.optimization_barrier((stats, packed, got))
    stats = lax.all_to_all(stats, ("sp_2", "tp"), 0, 0, tiled=True)
    send, own_rows, out_rows = call(
        outer_part,
        [like((rows, width), BF), like((rows, 2 * HEAD_DIM), BF), like((width, 2 * HEAD_DIM), BF)],
        where,
        (packed, inside, got, ret_gain.reshape(1, -1), stats, conv_gain.reshape(1, -1), others),
        [pltpu.VMEM((both_rows, 2 * HEAD_DIM), BF)],
        mib=14,
    )
    other = lax.ppermute(send, "sp_2", swap)
    keep = pl.pallas_call(
        keep_part,
        out_shape=like((rows, width), BF),
        in_specs=[pl.BlockSpec(memory_space=pltpu.VMEM)] * 2,
        out_specs=pl.BlockSpec(memory_space=pltpu.VMEM),
        compiler_params=pltpu.CompilerParams(vmem_limit_bytes=8 * 1024 * 1024),
        name="keep_part",
    )(own_rows, out_rows)
    partial = (keep.astype(F32) + other.astype(F32)).astype(BF)
    peers = lax.axis_size("tp")
    arrived = lax.all_to_all(partial.reshape(peers, rows // peers, width), "tp", 0, 0, tiled=True)
    return arrived.astype(F32).sum(axis=0).astype(BF)


def solution(mesh):
    finer = Mesh(mesh.devices.reshape(8, 8, 2, mesh.shape["tp"]), SP_TP)
    weight = P(SP, "tp")
    return jax.shard_map(
        per_device,
        mesh=finer,
        in_specs=(P(SP, None), P(), *[weight] * 8, P(), P(), P(), P("tp", SP)),
        out_specs=P(SP_TP, None),
        check_vma=False,
    )
```
